32 devices in a mesh: fs: 16 (over z, y, core), tp: 2 (over x).
Axes of the slice: x: 2, y: 2, z: 4, core: 2. Of those that a mesh axis runs over, the one named last changes fastest.
Arguments:
- tokens: bfloat16 [6144, 2048], P('fs', 'tp'), may hold values from -60 to 60
- gain_mixer: float32 [2048], P('tp'), may hold values from 0.1 to 1.9
- w_in: bfloat16 [2048, 1024], P('fs', 'tp'), may hold values from -0.125 to 0.125
- pool_scale: float32 [1024], P('tp'), may hold values from 0.1 to 1.9
- w_pool_out: bfloat16 [2048, 1024], P('fs', 'tp'), may hold values from -0.25 to 0.25
- gain_mid: float32 [2048], P('tp'), may hold values from 0.1 to 1.9
- w_ff1: bfloat16 [2048, 8192], P('fs', 'tp'), may hold values from -0.125 to 0.125
- w_ff2: bfloat16 [2048, 8192], P('fs', 'tp'), may hold values from -0.09375 to 0.09375
- gain_out: float32 [2048], P('tp'), may hold values from 0.1 to 1.9
Outputs:
- layer_out: bfloat16 [6144, 2048], P('fs', 'tp')
The draws below stay inside these ranges and needn't reach their ends.
All inputs are finite; a program needn't handle non-finite values.
Results may differ from the reference program's by a relative error of at most 0.017.
Values may be sent and summed in bfloat16 or wider, within the bound.
A program may use at most 128 MiB of HBM per device.

```python
import math
import jax
import jax.numpy as jnp
from jax import lax

D = 2048
POOL_WIDTH = 1024
FF = 8192
SEQ_DEV = 384
TOKENS = 6144
N_FS = 16
N_TP = 2


def draw_tokens(key, part):
    key_values = jax.random.fold_in(key, 11)
    key_rough = jax.random.fold_in(key, 12)
    column = jnp.arange(D, dtype=jnp.float32) / D
    rough = jax.random.uniform(key_rough, (D,), jnp.float32, 0.6, 1.5)
    scale = jnp.exp(math.log(4.0) * column) * rough
    values = jnp.clip(jax.random.normal(key_values, (TOKENS, D), jnp.float32), -6.0, 6.0)
    return (values * scale).astype(jnp.bfloat16)


def spiked(values, own_key, source, target, shards_of, factor):
    def block_of(dim):
        return (jnp.arange(values.shape[dim]) // (values.shape[dim] // shards_of)).reshape((-1,) + (1,) * (values.ndim - 1 - dim))

    first = jax.random.permutation(own_key, shards_of)[block_of(target)]
    second = (block_of(target) + shards_of // 2) % shards_of
    return jnp.where((block_of(source) == first) | (block_of(source) == second), factor * values, values)


def block_scale(key, dims, shards, low, top_value):
    factor_of, own = 1.0, jax.random.fold_in(key, 6)
    for dim, blocks in shards:
        heights = jnp.exp(jax.random.uniform(jax.random.fold_in(own, dim), (blocks,), jnp.float32, low / len(shards), top_value / len(shards)))
        factor_of = factor_of * jnp.repeat(heights, dims[dim] // blocks).reshape([-1 if axis == dim else 1 for axis in range(len(dims))])
    return factor_of


def noise(key, extent, scale, reach, split=(), kind=jnp.bfloat16):
    level = block_scale(key, extent, split, -0.22, 0.18) if split else 1.0
    drawn = jax.random.normal(key, extent, jnp.float32) * scale * level
    return jnp.minimum(jnp.maximum(drawn, -reach), reach).astype(kind)


def noise_with(key, shape, scale, bound, cuts, heavy, held_as=jnp.bfloat16):
    entries = scale * jax.random.normal(key, shape, jnp.float32)
    if cuts:
        entries = entries * block_scale(key, shape, cuts, -0.22, 0.18)
    return jnp.clip(spiked(entries, jax.random.fold_in(key, 3), *heavy), -bound, bound).astype(held_as)


def setup_inputs(seed: int = 0) -> dict:
    splits = jax.random.split(jax.random.key(seed), 10)
    return {
        "tokens": draw_tokens(jax.random.fold_in(splits[9], 71), 0),
        "gain_mixer": jnp.clip(1.0 + 0.18 * jax.random.normal(splits[1], (D,), jnp.float32), 0.1, 1.9),
        "w_in": noise(splits[2], (D, POOL_WIDTH), D ** -0.5, 0.125, ((0, 16), (1, 2))),
        "pool_scale": jnp.clip(1.0 + 0.18 * jax.random.normal(splits[3], (POOL_WIDTH,), jnp.float32), 0.1, 1.9),
        "w_pool_out": noise_with(splits[4], (D, POOL_WIDTH), POOL_WIDTH ** -0.5, 0.25, ((0, 16), (1, 2)), (1, 0, 16, 2.0)),
        "gain_mid": jnp.clip(1.0 + 0.18 * jax.random.normal(splits[5], (D,), jnp.float32), 0.1, 1.9),
        "w_ff1": noise(splits[6], (D, FF), D ** -0.5, 0.125, ((0, 16), (1, 2))),
        "w_ff2": noise_with(splits[7], (D, FF), FF ** -0.5, 0.09375, ((0, 16), (1, 2)), (1, 0, 16, 2.0)),
        "gain_out": jnp.clip(1.0 + 0.18 * jax.random.normal(splits[8], (D,), jnp.float32), 0.1, 1.9),
    }


norm_eps = 1e-05
residual_alpha = 2.0 ** 0.25

def norm_rows(value, gain):
    center = value - lax.optimization_barrier(jnp.mean(value, axis=-1, keepdims=True))
    spread = lax.optimization_barrier(jnp.mean(center * center, axis=-1, keepdims=True))
    return center * lax.rsqrt(spread + norm_eps) * gain

def block_sums(left, weight, blocks):
    width = left.shape[1] // blocks
    total = jnp.zeros((left.shape[0], weight.shape[0]), jnp.float32)
    for block in range(blocks):
        term = lax.dot_general(left[:, block * width:(block + 1) * width], weight[:, block * width:(block + 1) * width], (((1,), (1,)), ((), ())), preferred_element_type=jnp.float32)
        term = lax.optimization_barrier(term.astype(jnp.bfloat16))
        total = total + term.astype(jnp.float32)
    return total.astype(jnp.bfloat16)

def reference(tokens, gain_mixer, w_in, pool_scale, w_pool_out, gain_mid, w_ff1, w_ff2, gain_out):
    group = POOL_WIDTH // 4

    def one_sequence(seq_rows):
        xf = seq_rows.astype(jnp.float32)
        mixed_in = norm_rows(xf, gain_mixer).astype(jnp.bfloat16)
        pool_in = jnp.dot(mixed_in, w_in, preferred_element_type=jnp.float32).astype(jnp.bfloat16)
        uf = pool_in.astype(jnp.float32)
        length = uf.shape[0]
        sums = jnp.pad(jnp.cumsum(uf, axis=0), ((1, 0), (0, 0)))
        position = jnp.arange(length, dtype=jnp.float32)[:, None]
        pieces = []
        for index, window in enumerate((2, 4, 8, 16)):
            part = sums[:, index * group:(index + 1) * group]
            upper = part[1:]
            lower = jnp.pad(part, ((window - 1, 0), (0, 0)))[:length]
            count = jnp.minimum(position + 1.0, float(window))
            pieces.append((upper - lower) / count - uf[:, index * group:(index + 1) * group])
        pooled = (jnp.concatenate(pieces, axis=1) * pool_scale).astype(jnp.bfloat16)
        mixer_out = block_sums(pooled, w_pool_out, N_TP)
        middle = norm_rows(residual_alpha * xf + mixer_out.astype(jnp.float32), gain_mid).astype(jnp.bfloat16)
        upward = jnp.dot(middle, w_ff1, preferred_element_type=jnp.float32)
        hidden = jnp.square(jax.nn.relu(upward)).astype(jnp.bfloat16)
        ff_out = block_sums(hidden, w_ff2, N_TP)
        result = norm_rows(residual_alpha * middle.astype(jnp.float32) + ff_out.astype(jnp.float32), gain_out)
        return result.astype(jnp.bfloat16)
    stacked = tokens.reshape(N_FS, SEQ_DEV, D)
    return lax.map(one_sequence, stacked).reshape(N_FS * SEQ_DEV, D)
```

```python
import functools
import math

import jax
import jax.numpy as jnp
from jax import lax
from jax.experimental import pallas as pl
from jax.experimental.pallas import tpu as pltpu
from jax.sharding import PartitionSpec as P

norm_eps = 1e-05
residual_alpha = 2.0**0.25
f32, bf16 = jnp.float32, jnp.bfloat16
MESH = pl.DeviceIdType.MESH


def nt_dot(left, right):
    return lax.dot_general(left, right, (((1,), (1,)), ((), ())), preferred_element_type=f32)


def kernel(
    zn, tps,
    x_ref, gains_ref, scale_ref, gout_ref, win_ref, wpo_ref, wup_ref, wdn_ref, out_ref,
    win, wpo, wup, wdn, sup, sdn, xfull, gfull, mixed, mpart, mrecv, middle, hidden,
    part, precv, zpart, zrecv, total, moments, spread, stat, srecv, work,
    load_sem, zs_sem, zr_sem, ys_sem, yr_sem, ss_sem, sr_sem, xs_sem, xr_sem, gs_sem, gr_sem,
    ms_sem, mr_sem, as_sem, ar_sem, fs_sem, fr_sem, rs_sem, rr_sem, ps_sem, pr_sem, ts_sem, tr_sem,
):
    i, t = lax.axis_index("fs"), lax.axis_index("tp")
    c = lax.rem(i, 2)
    y = lax.rem(lax.div(i, 2), 2)
    z = lax.div(i, 4)
    role = lax.rem(z, 2)
    rows, feat = x_ref.shape
    cin = win_ref.shape[1]
    width = feat * tps
    own = win_ref.shape[0]
    ffw = wup_ref.shape[1]
    fh = ffw // 2
    fq = fh // 2
    n = zn * 2
    per = n // tps
    rc = own * 2
    hr = rows // 2
    lanes = tps - 1

    def across(j):
        other, bit = z, 1
        while bit < zn:
            if j & bit:
                other = other + bit * (1 - 2 * lax.rem(lax.div(z, bit), 2))
            bit *= 2
        return other

    order = [0]
    for j in range(1, zn // 2 + 1):
        for v in (zn // 2 + j - 1, j):
            if v not in order:
                order.append(v)
    far = order[1:]

    def dev(zz, yy, cc):
        return (zz * 2 + yy) * 2 + cc

    sib = dev(z, y, 1 - c)
    opp = dev(z, 1 - y, c)
    mate = dev(across(1), y, c)
    peers = [lax.rem(t + q, tps) for q in range(1, tps)]
    mine = pl.ds(pl.multiple_of(i * own, own), own)

    WIN, WPO, UP0, UP1, DN = range(5)
    streams = [(win, 0, cin), (wpo, 0, cin), (wup, 0, fq), (wup, fq, fq), (wdn, 0, fh)]

    def block(w, zz, yy, cc):
        ref, c0, cw = streams[w]
        r0 = pl.multiple_of(dev(zz, yy, cc) * own, own)
        return ref.at[pl.ds(r0, own), pl.ds(c0, cw)]

    def remote(src, dst, send, recv, to, tt):
        return pltpu.make_async_remote_copy(
            src, dst, send, recv, device_id=(to, tt), device_id_type=MESH)

    def zsend(w, j):
        zd = across(j)
        ref, c0, cw = streams[w]
        b = block(w, z, y, c)
        if w in (WIN, WPO):
            src = b
        else:
            stage = sdn if w == DN else sup
            src = stage.at[:, pl.ds(pl.multiple_of(lax.rem(zd, 2) * fh + c0, 128), cw)]
        return remote(src, b, zs_sem.at[w, j], zr_sem.at[w, j], dev(zd, y, c), t)

    def yfwd(w, j):
        b = block(w, across(j), y, c)
        return remote(b, b, ys_sem.at[w, j], yr_sem.at[w, j], opp, t)

    def share(w, j, s):
        b = block(w, across(j), y if s == 0 else 1 - y, c)
        return remote(b, b, ss_sem.at[w, j, s], sr_sem.at[w, j, s], sib, t)

    def zsends(w, js):
        for j in js:
            zsend(w, j).start()

    def own_start(w):
        yfwd(w, 0).start()
        share(w, 0, 0).start()

    def z_in(w, j):
        zsend(w, j).wait_recv()
        yfwd(w, j).start()
        share(w, j, 0).start()

    def y_in(w, j):
        yfwd(w, j).wait_recv()
        share(w, j, 1).start()

    def s_in(w):
        for j in order:
            for s in range(2):
                share(w, j, s).wait_recv()

    def x_copy(q):
        return remote(x_ref, xfull.at[t], xs_sem.at[q], xr_sem.at[q], i, peers[q])

    def g_copy(q):
        return remote(gains_ref, gfull.at[t], gs_sem.at[q], gr_sem.at[q], i, peers[q])

    def half(h):
        return pl.ds(h * hr, hr)

    def m_copy(q, h):
        return remote(mpart.at[half(h)], mrecv.at[q, half(h)], ms_sem.at[q, h], mr_sem.at[q, h], i, peers[q])

    slab = pl.ds(pl.multiple_of(t * feat, feat), feat)

    def a_copy(h):
        b = middle.at[role, half(h), slab]
        return remote(b, b, as_sem.at[h], ar_sem.at[h], mate, t)

    def f_copy(q, h):
        b = middle.at[1 - role, half(h), slab]
        return remote(b, b, fs_sem.at[q, h], fr_sem.at[q, h], i, peers[q])

    def slot(s):
        return pl.ds(pl.multiple_of(s * rows, rows), rows)

    def r_copy(g, s):
        holder, gl = lax.div(g, per), lax.rem(g, per)
        q = lax.rem(t - holder - 1 + 2 * tps, tps)
        which = (1 - role) if s == 0 else role
        return remote(
            part.at[g, slot(which)], precv.at[q, gl, slot(which)],
            rs_sem.at[g, s], rr_sem.at[q, gl, s], i, holder)

    def r_wait(q, gl, s):
        which = (1 - role) if s == 0 else role
        b = precv.at[q, gl, slot(which)]
        remote(b, b, rs_sem.at[0, s], rr_sem.at[q, gl, s], i, peers[0]).wait_recv()

    def p_copy(gl):
        return remote(zpart.at[gl], zrecv.at[gl], ps_sem.at[gl], pr_sem.at[gl], mate, t)

    def t_copy(q):
        return remote(stat, srecv.at[q], ts_sem.at[q], tr_sem.at[q], i, peers[q])

    barrier = pltpu.get_barrier_semaphore()
    for f in [dev(across(j), y, c) for j in far] + [opp, sib]:
        pl.semaphore_signal(barrier, inc=1, device_id=(f, t), device_id_type=MESH)
    for p in peers:
        pl.semaphore_signal(barrier, inc=1, device_id=(i, p), device_id_type=MESH)
    part_cols = pl.ds(pl.multiple_of(role * fh, 128), fh)
    loads = [
        pltpu.make_async_copy(win_ref, win.at[mine], load_sem.at[0]),
        pltpu.make_async_copy(wpo_ref, wpo.at[mine], load_sem.at[1]),
        pltpu.make_async_copy(wup_ref, sup, load_sem.at[2]),
        pltpu.make_async_copy(wup_ref.at[:, part_cols], wup.at[mine], load_sem.at[3]),
        pltpu.make_async_copy(wdn_ref, sdn, load_sem.at[4]),
        pltpu.make_async_copy(wdn_ref.at[:, part_cols], wdn.at[mine], load_sem.at[5]),
    ]
    for copy in loads:
        copy.start()
    pl.semaphore_wait(barrier, len(far) + 2 + len(peers))

    for q in range(lanes):
        x_copy(q).start()
        g_copy(q).start()
    loads[0].wait()
    own_start(WIN)
    zsends(WIN, far)
    loads[1].wait()
    own_start(WPO)
    zsends(WPO, far)
    loads[2].wait()
    loads[3].wait()
    zsends(UP0, far)
    xfull[t] = x_ref[...]
    gfull[t] = gains_ref[...]
    loads[4].wait()
    loads[5].wait()

    rb = math.gcd(hr, 32)

    def blocks_of(body, lo=0, hi=rows):
        def step(r, carry):
            body(pl.ds(pl.multiple_of(lo + r * rb, rb), rb))
            return carry
        lax.fori_loop(0, (hi - lo) // rb, step, 0)

    def norm(pieces):
        mean = sum(jnp.sum(v, axis=1, keepdims=True) for v in pieces) / width
        pieces = [v - mean for v in pieces]
        var = sum(jnp.sum(v * v, axis=1, keepdims=True) for v in pieces) / width
        inv = lax.rsqrt(var + norm_eps)
        return [v * inv for v in pieces]

    def first_norm(rs):
        pieces = norm([xfull[r, rs, :].astype(f32) for r in range(tps)])
        for r in range(tps):
            mixed[rs, r * feat:(r + 1) * feat] = (pieces[r] * gfull[r, 0:1, :]).astype(bf16)

    zev = [(WIN, j) for j in far] + [(WPO, j) for j in far]
    yev = [(WIN, 0), (WPO, 0)] + zev
    for k, ev in enumerate(zev):
        z_in(*ev)
        if k >= 1:
            y_in(*yev[k - 1])
        if k == len(far):
            for q in range(lanes):
                x_copy(q).wait_recv()
                g_copy(q).wait_recv()
            blocks_of(first_norm)
    own_start(UP0)
    own_start(UP1)
    zsends(UP1, far)
    rest = yev[len(zev) - 1:]
    for ev in rest:
        if ev[0] == WIN:
            y_in(*ev)
    rest = [ev for ev in rest if ev[0] == WPO]
    s_in(WIN)

    cb = math.gcd(cin, 128)
    gw = cin * tps // 4
    pool = jnp.dot(mixed[...], win[...], preferred_element_type=f32)
    work[:, :cin] = pool.astype(bf16).astype(f32)
    for ev in rest:
        y_in(*ev)
    row = lax.broadcasted_iota(jnp.int32, (rows, cb), 0)
    position = (row + 1).astype(f32)
    for k in range(cin // cb):
        cs = slice(k * cb, (k + 1) * cb)
        u = work[:, cs]

        def shifted(v, steps):
            return jnp.where(row >= steps, pltpu.roll(v, steps, axis=0), 0.0)

        s2 = u + shifted(u, 1)
        s4 = s2 + shifted(s2, 2)
        s8 = s4 + shifted(s4, 4)
        s16 = s8 + shifted(s8, 8)
        channel = t * cin + k * cb + lax.broadcasted_iota(jnp.int32, (rows, cb), 1)

        def pick(a, b, e, g):
            return jnp.where(channel < gw, a, jnp.where(channel < 2 * gw, b, jnp.where(channel < 3 * gw, e, g)))

        count = jnp.minimum(position, pick(2.0, 4.0, 8.0, 16.0))
        mixed[:, cs] = ((pick(s2, s4, s8, s16) / count - u) * scale_ref[0:1, cs]).astype(bf16)

    s_in(WPO)
    wb = math.gcd(width, 512)
    for h in range(2):
        def out_proj(k, carry):
            cs = pl.ds(pl.multiple_of(k * wb, wb), wb)
            mpart[half(h), cs] = nt_dot(mixed[half(h), :cin], wpo[cs, :]).astype(bf16)
            return carry

        lax.fori_loop(0, width // wb, out_proj, 0)
        for q in range(lanes):
            m_copy(q, h).start()

    def second_norm(rs):
        pieces = []
        for r in range(tps):
            cs = slice(r * feat, (r + 1) * feat)
            mix = mpart[rs, cs].astype(f32)
            for q in range(lanes):
                mix = mix + mrecv[q, rs, cs].astype(f32)
            mix = mix.astype(bf16).astype(f32)
            pieces.append(residual_alpha * xfull[r, rs, :].astype(f32) + mix)
        pieces = norm(pieces)
        for r in range(tps):
            middle[role, rs, r * feat:(r + 1) * feat] = (pieces[r] * gfull[r, 1:2, :]).astype(bf16)

    def settle(h):
        for q in range(lanes):
            m_copy(q, h).wait_recv()
        blocks_of(second_norm, h * hr, (h + 1) * hr)
        a_copy(h).start()

    zev = [(UP0, j) for j in far] + [(UP1, j) for j in far]
    yev = [(UP0, 0), (UP1, 0)] + zev
    for k, ev in enumerate(zev):
        z_in(*ev)
        y_in(*yev[k])
        if k == len(far):
            settle(0)
        if k == len(far) + 1:
            own_start(DN)
            zsends(DN, far[:1])
    settle(1)
    zsends(DN, far[1:])
    for ev in yev[len(zev):]:
        y_in(*ev)

    hb = math.gcd(fq, 512)

    def ff1(s, lo, hi):
        def up(k, carry):
            cs = pl.ds(pl.multiple_of(lo + k * hb, hb), hb)
            act = jnp.maximum(jnp.dot(middle[s], wup[:, cs], preferred_element_type=f32), 0.0)
            hidden[slot(s), cs] = (act * act).astype(bf16)
            return carry
        lax.fori_loop(0, (hi - lo) // hb, up, 0)

    def pass_on(h):
        a_back = middle.at[1 - role, half(h), slab]
        remote(a_back, a_back, as_sem.at[h], ar_sem.at[h], mate, t).wait_recv()
        for q in range(lanes):
            f_copy(q, h).start()

    s_in(UP0)
    ff1(role, 0, fq)
    pass_on(0)
    z_in(DN, far[0])
    s_in(UP1)
    ff1(role, fq, fh)
    pass_on(1)
    y_in(DN, 0)
    for h in range(2):
        for q in range(lanes):
            f_copy(q, h).wait_recv()
    ff1(1 - role, 0, fh)

    def down(j, s):
        g = across(j) * 2 + (y if s == 0 else 1 - y)
        share(DN, j, s).wait_recv()
        part[g] = nt_dot(hidden[...], wdn[pl.ds(pl.multiple_of(g * rc, rc), rc), :]).astype(bf16)

        @pl.when(lax.div(g, per) != t)
        def _():
            r_copy(g, 0).start()
            r_copy(g, 1).start()

    def fold(j, s):
        g = across(j) * 2 + (y if s == 0 else 1 - y)
        gl = lax.rem(g, per)

        @pl.when(lax.div(g, per) == t)
        def _():
            for q in range(lanes):
                r_wait(q, gl, 0)
            v = part[g, slot(1 - role), :].astype(f32)
            for q in range(lanes):
                v = v + precv[q, gl, slot(1 - role), :].astype(f32)
            zpart[gl] = v.astype(bf16)
            p_copy(gl).start()

    for k, j in enumerate(order):
        if k + 2 < zn:
            z_in(DN, order[k + 2])
        down(j, 0)
        if k + 1 < zn:
            y_in(DN, order[k + 1])
        down(j, 1)
        if k:
            for s in range(2):
                fold(order[k - 1], s)
    for s in range(2):
        fold(order[-1], s)

    for gl in range(per):
        for q in range(lanes):
            r_wait(q, gl, 1)
        p_copy(gl).wait_recv()

    lane = lax.broadcasted_iota(jnp.int32, (rb, 128), 1)

    def gather_up(rs):
        own_rows = pl.ds(pl.multiple_of(role * rows + rs.start, rb), rb)
        base = middle[role, rs, slab]
        values = []
        mean = jnp.zeros((rb, 1), f32)
        for gl in range(per):
            ff = part[t * per + gl, own_rows, :].astype(f32)
            for q in range(lanes):
                ff = ff + precv[q, gl, own_rows, :].astype(f32)
            ff = (ff + zrecv[gl, rs, :].astype(f32)).astype(bf16).astype(f32)
            v = residual_alpha * base[:, gl * rc:(gl + 1) * rc].astype(f32) + ff
            total[rs, gl * rc:(gl + 1) * rc] = v
            values.append(v)
            mean = mean + jnp.sum(v, axis=1, keepdims=True)
        mean = mean / feat
        square = jnp.zeros((rb, 1), f32)
        for v in values:
            square = square + jnp.sum((v - mean) * (v - mean), axis=1, keepdims=True)
        moments[0, rs, :] = jnp.where(lane == 0, mean, jnp.where(lane == 1, square, 0.0))

    blocks_of(gather_up)
    stat[...] = jnp.transpose(moments[0])[0:8, :]
    for q in range(lanes):
        t_copy(q).start()
    spread[...] = jnp.zeros_like(spread)
    for q in range(lanes):
        t_copy(q).wait_recv()
        spread[0:8, :] = srecv[q]
        moments[q + 1] = jnp.transpose(spread[...])

    def last_norm(rs):
        means = [moments[q, rs, 0:1] for q in range(tps)]
        mean = sum(means) / tps
        square = sum(moments[q, rs, 1:2] for q in range(tps))
        for m in means:
            square = square + feat * (m - mean) * (m - mean)
        inv = lax.rsqrt(square / width + norm_eps)
        out_ref[rs, :] = ((total[rs, :] - mean) * inv * gout_ref[0:1, :]).astype(bf16)

    blocks_of(last_norm)

    for q in range(lanes):
        x_copy(q).wait_send()
        g_copy(q).wait_send()
        t_copy(q).wait_send()
        for h in range(2):
            m_copy(q, h).wait_send()
            f_copy(q, h).wait_send()
    for h in range(2):
        a_copy(h).wait_send()

    def sent(g, carry):
        @pl.when(lax.div(g, per) != t)
        def _():
            r_copy(g, 0).wait_send()
            r_copy(g, 1).wait_send()
        return carry

    lax.fori_loop(0, n, sent, 0)

    def folded(gl, carry):
        p_copy(gl).wait_send()
        return carry

    lax.fori_loop(0, per, folded, 0)
    for w in range(len(streams)):
        for j in order:
            if j:
                zsend(w, j).wait_send()
            yfwd(w, j).wait_send()
            share(w, j, 0).wait_send()
            share(w, j, 1).wait_send()


def local(zn, tps, tokens, gain_mixer, w_in, pool_scale, w_pool_out, gain_mid, w_ff1, w_ff2, gain_out):
    rows, feat = tokens.shape
    own, cin = w_in.shape
    ffw = w_ff1.shape[1]
    fh = ffw // 2
    width = feat * tps
    n = zn * 2
    per = n // tps
    rc = own * 2
    gains = jnp.stack([gain_mixer, gain_mid])
    vmem, hbm = pl.BlockSpec(memory_space=pltpu.VMEM), pl.BlockSpec(memory_space=pl.ANY)
    dma = pltpu.SemaphoreType.DMA
    lanes = tps - 1
    return pl.pallas_call(
        functools.partial(kernel, zn, tps),
        out_shape=jax.ShapeDtypeStruct((rows, feat), bf16),
        in_specs=[vmem] * 4 + [hbm] * 4,
        out_specs=vmem,
        scratch_shapes=[
            pltpu.VMEM((width, cin), bf16),
            pltpu.VMEM((width, cin), bf16),
            pltpu.VMEM((width, fh), bf16),
            pltpu.VMEM((width, fh), bf16),
            pltpu.VMEM((own, ffw), bf16),
            pltpu.VMEM((own, ffw), bf16),
            pltpu.VMEM((tps, rows, feat), bf16),
            pltpu.VMEM((tps, 2, feat), f32),
            pltpu.VMEM((rows, width), bf16),
            pltpu.VMEM((rows, width), bf16),
            pltpu.VMEM((lanes, rows, width), bf16),
            pltpu.VMEM((2, rows, width), bf16),
            pltpu.VMEM((2 * rows, fh), bf16),
            pltpu.VMEM((n, 2 * rows, rc), bf16),
            pltpu.VMEM((lanes, per, 2 * rows, rc), bf16),
            pltpu.VMEM((per, rows, rc), bf16),
            pltpu.VMEM((per, rows, rc), bf16),
            pltpu.VMEM((rows, feat), f32),
            pltpu.VMEM((tps, rows, 128), f32),
            pltpu.VMEM((128, rows), f32),
            pltpu.VMEM((8, rows), f32),
            pltpu.VMEM((lanes, 8, rows), f32),
            pltpu.VMEM((rows, cin), f32),
            dma((6,)),
            dma((5, zn)), dma((5, zn)), dma((5, zn)), dma((5, zn)), dma((5, zn, 2)), dma((5, zn, 2)),
            dma((lanes,)), dma((lanes,)), dma((lanes,)), dma((lanes,)),
            dma((lanes, 2)), dma((lanes, 2)), dma((2,)), dma((2,)), dma((lanes, 2)), dma((lanes, 2)),
            dma((n, 2)), dma((lanes, per, 2)), dma((per,)), dma((per,)), dma((lanes,)), dma((lanes,)),
        ],
        compiler_params=pltpu.CompilerParams(
            collective_id=0, has_side_effects=True, vmem_limit_bytes=67043328
        ),
    )(tokens, gains, pool_scale[None], gain_out[None], w_in, w_pool_out, w_ff1, w_ff2)


def solution(mesh):
    zn, tps = mesh.shape["fs"] // 4, mesh.shape["tp"]
    return jax.shard_map(
        functools.partial(local, zn, tps),
        mesh=mesh,
        in_specs=(
            P("fs", "tp"),
            P("tp"),
            P("fs", "tp"),
            P("tp"),
            P("fs", "tp"),
            P("tp"),
            P("fs", "tp"),
            P("fs", "tp"),
            P("tp"),
        ),
        out_specs=P("fs", "tp"),
        check_vma=False,
    )
```

```python
import functools
import math

import jax
import jax.numpy as jnp
from jax import lax
from jax.experimental import pallas as pl
from jax.experimental.pallas import tpu as pltpu
from jax.sharding import PartitionSpec as P

norm_eps = 1e-05
residual_alpha = 2.0**0.25
f32, bf16 = jnp.float32, jnp.bfloat16
MESH = pl.DeviceIdType.MESH
scope = jax.named_scope


def nt_dot(left, right):
    return lax.dot_general(left, right, (((1,), (1,)), ((), ())), preferred_element_type=f32)


def kernel(
    zn, tps,
    x_ref, gains_ref, scale_ref, gout_ref, win_ref, wpo_ref, wup_ref, wdn_ref, out_ref,
    win, wpo, wup, wdn, sup, sdn, xfull, gfull, mixed, mpart, mrecv, middle, hidden,
    part, precv, zpart, zrecv, total, moments, spread, stat, srecv, work,
    load_sem, zs_sem, zq_sem, zr_sem, ys_sem, yr_sem, ss_sem, sr_sem, xs_sem, xr_sem, gs_sem, gr_sem,
    ms_sem, mr_sem, as_sem, ar_sem, fs_sem, fr_sem, rs_sem, rr_sem, ps_sem, pr_sem, ts_sem, tr_sem,
):
    i, t = lax.axis_index("fs"), lax.axis_index("tp")
    c = lax.rem(i, 2)
    y = lax.rem(lax.div(i, 2), 2)
    z = lax.div(i, 4)
    role = lax.rem(z, 2)
    rows, feat = x_ref.shape
    cin = win_ref.shape[1]
    width = feat * tps
    own = win_ref.shape[0]
    ffw = wup_ref.shape[1]
    fh = ffw // 2
    fq = fh // 2
    n = zn * 2
    per = n // tps
    rc = own * 2
    hr = rows // 2
    lanes = tps - 1

    def across(j):
        other, bit = z, 1
        while bit < zn:
            if j & bit:
                other = other + bit * (1 - 2 * lax.rem(lax.div(z, bit), 2))
            bit *= 2
        return other

    order = [0]
    for j in range(1, zn // 2 + 1):
        for v in (zn // 2 + j - 1, j):
            if v not in order:
                order.append(v)
    far = order[1:]
    near = [1] + [v for j in range(2, zn, 2) for v in (j + 1, j)]

    def dev(zz, yy, cc):
        return (zz * 2 + yy) * 2 + cc

    sib = dev(z, y, 1 - c)
    opp = dev(z, 1 - y, c)
    mate = dev(across(1), y, c)
    peers = [lax.rem(t + q, tps) for q in range(1, tps)]
    mine = pl.ds(pl.multiple_of(i * own, own), own)

    WIN, WPO, UP0, UP1, DN = range(5)
    streams = [(win, 0, cin), (wpo, 0, cin), (wup, 0, fq), (wup, fq, fq), (wdn, 0, fh)]

    def block(w, zz, yy, cc):
        ref, c0, cw = streams[w]
        r0 = pl.multiple_of(dev(zz, yy, cc) * own, own)
        return ref.at[pl.ds(r0, own), pl.ds(c0, cw)]

    def remote(src, dst, send, recv, to, tt):
        return pltpu.make_async_remote_copy(
            src, dst, send, recv, device_id=(to, tt), device_id_type=MESH)

    def zsend(w, j):
        zd = across(j)
        ref, c0, cw = streams[w]
        b = block(w, z, y, c)
        if w in (WIN, WPO):
            src = b
        else:
            stage = sdn if w == DN else sup
            src = stage.at[:, pl.ds(pl.multiple_of(lax.rem(zd, 2) * fh + c0, 128), cw)]
        return remote(src, b, zs_sem.at[w, j], zr_sem.at[w, j], dev(zd, y, c), t)

    def yfwd(w, j):
        b = block(w, across(j), y, c)
        return remote(b, b, ys_sem.at[w, j], yr_sem.at[w, j], opp, t)

    def share(w, j, s):
        b = block(w, across(j), y if s == 0 else 1 - y, c)
        return remote(b, b, ss_sem.at[w, j, s], sr_sem.at[w, j, s], sib, t)

    def zsends(w, js):
        for j in js:
            zsend(w, j).start()

    def gate(me, other):
        lower = lax.rem(me, 2) == 0
        before = lax.div(other, 2) < lax.div(me, 2)
        return (lower & before) | (~lower & ~before)

    def relay(w, j):
        b = block(w, across(j), y, c)
        return remote(b, b, zq_sem.at[w, j], zr_sem.at[w, j ^ 1], mate, t)

    def spread_out(w):
        zsend(w, 1).start()
        for j in near[1:]:
            @pl.when(gate(across(j), z))
            def _():
                zsend(w, j).start()

    def own_start(w):
        yfwd(w, 0).start()
        share(w, 0, 0).start()

    def z_in(w, j):
        with scope(f"z{w}_{j}"):
            zsend(w, j).wait_recv()
        if w in (WIN, WPO) and j > 1:
            @pl.when(gate(z, across(j)))
            def _():
                relay(w, j).start()
        yfwd(w, j).start()
        share(w, j, 0).start()

    def y_in(w, j):
        with scope(f"y{w}_{j}"):
            yfwd(w, j).wait_recv()
        share(w, j, 1).start()

    def s_in(w):
        with scope(f"s{w}"):
            for j in order:
                for s in range(2):
                    share(w, j, s).wait_recv()

    def x_copy(q):
        return remote(x_ref, xfull.at[t], xs_sem.at[q], xr_sem.at[q], i, peers[q])

    def g_copy(q):
        return remote(gains_ref, gfull.at[t], gs_sem.at[q], gr_sem.at[q], i, peers[q])

    def half(h):
        return pl.ds(h * hr, hr)

    def m_copy(q, h):
        return remote(mpart.at[half(h)], mrecv.at[q, half(h)], ms_sem.at[q, h], mr_sem.at[q, h], i, peers[q])

    slab = pl.ds(pl.multiple_of(t * feat, feat), feat)

    def a_copy(h):
        b = middle.at[role, half(h), slab]
        return remote(b, b, as_sem.at[h], ar_sem.at[h], mate, t)

    def f_copy(q, h):
        b = middle.at[1 - role, half(h), slab]
        return remote(b, b, fs_sem.at[q, h], fr_sem.at[q, h], i, peers[q])

    def slot(s):
        return pl.ds(pl.multiple_of(s * rows, rows), rows)

    def r_copy(g, s):
        holder, gl = lax.div(g, per), lax.rem(g, per)
        q = lax.rem(t - holder - 1 + 2 * tps, tps)
        which = (1 - role) if s == 0 else role
        return remote(
            part.at[g, slot(which)], precv.at[q, gl, slot(which)],
            rs_sem.at[g, s], rr_sem.at[q, gl, s], i, holder)

    def r_wait(q, gl, s):
        which = (1 - role) if s == 0 else role
        b = precv.at[q, gl, slot(which)]
        remote(b, b, rs_sem.at[0, s], rr_sem.at[q, gl, s], i, peers[0]).wait_recv()

    def p_copy(gl):
        return remote(zpart.at[gl], zrecv.at[gl], ps_sem.at[gl], pr_sem.at[gl], mate, t)

    def t_copy(q):
        return remote(stat, srecv.at[q], ts_sem.at[q], tr_sem.at[q], i, peers[q])

    barrier = pltpu.get_barrier_semaphore()
    for f in [dev(across(j), y, c) for j in far] + [opp, sib]:
        pl.semaphore_signal(barrier, inc=1, device_id=(f, t), device_id_type=MESH)
    for p in peers:
        pl.semaphore_signal(barrier, inc=1, device_id=(i, p), device_id_type=MESH)
    part_cols = pl.ds(pl.multiple_of(role * fh, 128), fh)
    loads = [
        pltpu.make_async_copy(win_ref, win.at[mine], load_sem.at[0]),
        pltpu.make_async_copy(wpo_ref, wpo.at[mine], load_sem.at[1]),
        pltpu.make_async_copy(wup_ref, sup, load_sem.at[2]),
        pltpu.make_async_copy(wup_ref.at[:, part_cols], wup.at[mine], load_sem.at[3]),
        pltpu.make_async_copy(wdn_ref, sdn, load_sem.at[4]),
        pltpu.make_async_copy(wdn_ref.at[:, part_cols], wdn.at[mine], load_sem.at[5]),
    ]
    for copy in loads:
        copy.start()
    with scope("begin"):
        pl.semaphore_wait(barrier, len(far) + 2 + len(peers))

    for q in range(lanes):
        x_copy(q).start()
        g_copy(q).start()
    loads[0].wait()
    own_start(WIN)
    spread_out(WIN)
    loads[1].wait()
    own_start(WPO)
    spread_out(WPO)
    loads[2].wait()
    loads[3].wait()
    xfull[t] = x_ref[...]
    gfull[t] = gains_ref[...]
    loads[4].wait()
    loads[5].wait()

    rb = math.gcd(hr, 32)

    def blocks_of(body, lo=0, hi=rows):
        def step(r, carry):
            body(pl.ds(pl.multiple_of(lo + r * rb, rb), rb))
            return carry
        lax.fori_loop(0, (hi - lo) // rb, step, 0)

    def norm(pieces):
        mean = sum(jnp.sum(v, axis=1, keepdims=True) for v in pieces) / width
        pieces = [v - mean for v in pieces]
        var = sum(jnp.sum(v * v, axis=1, keepdims=True) for v in pieces) / width
        inv = lax.rsqrt(var + norm_eps)
        return [v * inv for v in pieces]

    def first_norm(rs):
        pieces = norm([xfull[r, rs, :].astype(f32) for r in range(tps)])
        for r in range(tps):
            mixed[rs, r * feat:(r + 1) * feat] = (pieces[r] * gfull[r, 0:1, :]).astype(bf16)

    mids = [j for j in far if j > 1]

    def wave(w, first):
        for j in mids:
            ahead = gate(across(j), z)

            @pl.when(ahead if first else ~ahead)
            def _():
                zsend(w, j).start()

    for w in (WIN, WPO):
        for j in near:
            z_in(w, j)
    wave(UP0, True)
    y_in(WIN, 0)
    y_in(WPO, 0)
    for j in near[:-1]:
        y_in(WIN, j)
    with scope("xwait"):
        for q in range(lanes):
            x_copy(q).wait_recv()
            g_copy(q).wait_recv()
    with scope("norm1"):
        blocks_of(first_norm)
    wave(UP0, False)
    zsends(UP0, [1])
    own_start(UP0)
    y_in(WIN, near[-1])
    y_in(WPO, near[0])
    s_in(WIN)

    cb = math.gcd(cin, 128)
    gw = cin * tps // 4
    with scope("pooldot"):
        pool = jnp.dot(mixed[...], win[...], preferred_element_type=f32)
        work[:, :cin] = pool.astype(bf16).astype(f32)
    for j in near[1:-1]:
        y_in(WPO, j)
    row = lax.broadcasted_iota(jnp.int32, (rows, cb), 0)
    position = (row + 1).astype(f32)
    for k in range(cin // cb):
        cs = slice(k * cb, (k + 1) * cb)
        u = work[:, cs]

        def shifted(v, steps):
            return jnp.where(row >= steps, pltpu.roll(v, steps, axis=0), 0.0)

        s2 = u + shifted(u, 1)
        s4 = s2 + shifted(s2, 2)
        s8 = s4 + shifted(s4, 4)
        s16 = s8 + shifted(s8, 8)
        channel = t * cin + k * cb + lax.broadcasted_iota(jnp.int32, (rows, cb), 1)

        def pick(a, b, e, g):
            return jnp.where(channel < gw, a, jnp.where(channel < 2 * gw, b, jnp.where(channel < 3 * gw, e, g)))

        count = jnp.minimum(position, pick(2.0, 4.0, 8.0, 16.0))
        mixed[:, cs] = ((pick(s2, s4, s8, s16) / count - u) * scale_ref[0:1, cs]).astype(bf16)

    y_in(WPO, near[-1])
    own_start(UP1)
    s_in(WPO)
    wb = math.gcd(width, 512)
    for h in range(2):
        def out_proj(k, carry):
            cs = pl.ds(pl.multiple_of(k * wb, wb), wb)
            mpart[half(h), cs] = nt_dot(mixed[half(h), :cin], wpo[cs, :]).astype(bf16)
            return carry

        with scope("outproj"):
            lax.fori_loop(0, width // wb, out_proj, 0)
        for q in range(lanes):
            m_copy(q, h).start()

    def second_norm(rs):
        pieces = []
        for r in range(tps):
            cs = slice(r * feat, (r + 1) * feat)
            mix = mpart[rs, cs].astype(f32)
            for q in range(lanes):
                mix = mix + mrecv[q, rs, cs].astype(f32)
            mix = mix.astype(bf16).astype(f32)
            pieces.append(residual_alpha * xfull[r, rs, :].astype(f32) + mix)
        pieces = norm(pieces)
        for r in range(tps):
            middle[role, rs, r * feat:(r + 1) * feat] = (pieces[r] * gfull[r, 1:2, :]).astype(bf16)

    def settle(h):
        with scope("mwait"):
            for q in range(lanes):
                m_copy(q, h).wait_recv()
        with scope("norm2"):
            blocks_of(second_norm, h * hr, (h + 1) * hr)
        a_copy(h).start()

    wave(UP1, True)
    zsends(UP1, [1])
    z_in(UP0, 1)
    y_in(UP0, 0)
    for j in mids:
        z_in(UP0, j)
    wave(UP1, False)
    y_in(UP1, 0)
    y_in(UP0, 1)
    settle(0)
    for j in mids[:-1]:
        y_in(UP0, j)
    zsends(DN, mids[:1])
    z_in(UP1, 1)
    y_in(UP0, mids[-1])
    for j in mids:
        z_in(UP1, j)
    own_start(DN)
    settle(1)
    zsends(DN, [1])
    hb = math.gcd(fq, 512)

    def ff1(s, lo, hi):
        def up(k, carry):
            cs = pl.ds(pl.multiple_of(lo + k * hb, hb), hb)
            act = jnp.maximum(jnp.dot(middle[s], wup[:, cs], preferred_element_type=f32), 0.0)
            hidden[slot(s), cs] = (act * act).astype(bf16)
            return carry
        with scope("ff1"):
            lax.fori_loop(0, (hi - lo) // hb, up, 0)

    def pass_on(h):
        a_back = middle.at[1 - role, half(h), slab]
        with scope("await"):
            remote(a_back, a_back, as_sem.at[h], ar_sem.at[h], mate, t).wait_recv()
        for q in range(lanes):
            f_copy(q, h).start()

    y_in(UP1, 1)
    pass_on(0)
    for j in mids[:-1]:
        y_in(UP1, j)
    s_in(UP0)
    ff1(role, 0, fq)
    y_in(UP1, mids[-1])
    s_in(UP1)
    ff1(role, fq, fh)
    zsends(DN, mids[1:])
    pass_on(1)

    def group(j, s):
        return across(j) * 2 + (y if s == 0 else 1 - y)

    landed = []

    def down(j, s, kept):
        g = group(j, s)
        which = role if kept else 1 - role
        if (j, s) not in landed:
            landed.append((j, s))
            with scope(f"dshare{j}_{s}"):
                share(DN, j, s).wait_recv()
        with scope("ff2"):
            w = wdn[pl.ds(pl.multiple_of(g * rc, rc), rc), :]
            part[g, slot(which), :] = nt_dot(hidden[slot(which), :], w).astype(bf16)

        @pl.when(lax.div(g, per) != t)
        def _():
            r_copy(g, 1 if kept else 0).start()

    down(0, 0, True)
    y_in(DN, 0)
    z_in(DN, far[0])
    down(0, 1, True)
    down(far[0], 0, True)
    with scope("fwait"):
        for h in range(2):
            for q in range(lanes):
                f_copy(q, h).wait_recv()
    ff1(1 - role, 0, fh)
    for ev in ((0, 0), (0, 1), (far[0], 0)):
        down(*ev, False)
    z_in(DN, far[1])
    y_in(DN, far[0])

    def fold(j, s):
        g = across(j) * 2 + (y if s == 0 else 1 - y)
        gl = lax.rem(g, per)

        @pl.when(lax.div(g, per) == t)
        def _():
            with scope(f"rwait{j}_{s}"):
                for q in range(lanes):
                    r_wait(q, gl, 0)
            v = part[g, slot(1 - role), :].astype(f32)
            for q in range(lanes):
                v = v + precv[q, gl, slot(1 - role), :].astype(f32)
            zpart[gl] = v.astype(bf16)
            p_copy(gl).start()

    def both(j, s):
        down(j, s, False)
        down(j, s, True)

    both(far[0], 1)
    both(far[1], 0)
    pending = [(0, 0), (0, 1), (far[0], 0), (far[0], 1), (far[1], 0)]
    for k in range(1, len(far)):
        if k + 1 < len(far):
            z_in(DN, far[k + 1])
        for ev in pending[:2]:
            fold(*ev)
        pending = pending[2:]
        y_in(DN, far[k])
        both(far[k], 1)
        pending.append((far[k], 1))
        if k + 1 < len(far):
            both(far[k + 1], 0)
            pending.append((far[k + 1], 0))
    for ev in pending:
        fold(*ev)

    for gl in range(per):
        with scope(f"r1wait{gl}"):
            for q in range(lanes):
                r_wait(q, gl, 1)
        with scope(f"pwait{gl}"):
            p_copy(gl).wait_recv()

    lane = lax.broadcasted_iota(jnp.int32, (rb, 128), 1)

    def gather_up(rs):
        own_rows = pl.ds(pl.multiple_of(role * rows + rs.start, rb), rb)
        base = middle[role, rs, slab]
        values = []
        mean = jnp.zeros((rb, 1), f32)
        for gl in range(per):
            ff = part[t * per + gl, own_rows, :].astype(f32)
            for q in range(lanes):
                ff = ff + precv[q, gl, own_rows, :].astype(f32)
            ff = (ff + zrecv[gl, rs, :].astype(f32)).astype(bf16).astype(f32)
            v = residual_alpha * base[:, gl * rc:(gl + 1) * rc].astype(f32) + ff
            total[rs, gl * rc:(gl + 1) * rc] = v
            values.append(v)
            mean = mean + jnp.sum(v, axis=1, keepdims=True)
        mean = mean / feat
        square = jnp.zeros((rb, 1), f32)
        for v in values:
            square = square + jnp.sum((v - mean) * (v - mean), axis=1, keepdims=True)
        moments[0, rs, :] = jnp.where(lane == 0, mean, jnp.where(lane == 1, square, 0.0))

    with scope("gather_up"):
        blocks_of(gather_up)
    stat[...] = jnp.transpose(moments[0])[0:8, :]
    for q in range(lanes):
        t_copy(q).start()
    spread[...] = jnp.zeros_like(spread)
    for q in range(lanes):
        with scope("twait"):
            t_copy(q).wait_recv()
        spread[0:8, :] = srecv[q]
        moments[q + 1] = jnp.transpose(spread[...])

    def last_norm(rs):
        means = [moments[q, rs, 0:1] for q in range(tps)]
        mean = sum(means) / tps
        square = sum(moments[q, rs, 1:2] for q in range(tps))
        for m in means:
            square = square + feat * (m - mean) * (m - mean)
        inv = lax.rsqrt(square / width + norm_eps)
        out_ref[rs, :] = ((total[rs, :] - mean) * inv * gout_ref[0:1, :]).astype(bf16)

    with scope("norm3"):
        blocks_of(last_norm)

    for q in range(lanes):
        x_copy(q).wait_send()
        g_copy(q).wait_send()
        t_copy(q).wait_send()
        for h in range(2):
            m_copy(q, h).wait_send()
            f_copy(q, h).wait_send()
    for h in range(2):
        a_copy(h).wait_send()

    def sent(g, carry):
        @pl.when(lax.div(g, per) != t)
        def _():
            r_copy(g, 0).wait_send()
            r_copy(g, 1).wait_send()
        return carry

    lax.fori_loop(0, n, sent, 0)

    def folded(gl, carry):
        p_copy(gl).wait_send()
        return carry

    lax.fori_loop(0, per, folded, 0)
    for w in range(len(streams)):
        for j in order:
            if j == 1 or (j and w not in (WIN, WPO)):
                zsend(w, j).wait_send()
            elif j:
                @pl.when(gate(across(j), z))
                def _():
                    zsend(w, j).wait_send()

                @pl.when(gate(z, across(j)))
                def _():
                    relay(w, j).wait_send()
            yfwd(w, j).wait_send()
            share(w, j, 0).wait_send()
            share(w, j, 1).wait_send()


def local(zn, tps, tokens, gain_mixer, w_in, pool_scale, w_pool_out, gain_mid, w_ff1, w_ff2, gain_out):
    rows, feat = tokens.shape
    own, cin = w_in.shape
    ffw = w_ff1.shape[1]
    fh = ffw // 2
    width = feat * tps
    n = zn * 2
    per = n // tps
    rc = own * 2
    gains = jnp.stack([gain_mixer, gain_mid])
    vmem, hbm = pl.BlockSpec(memory_space=pltpu.VMEM), pl.BlockSpec(memory_space=pl.ANY)
    dma = pltpu.SemaphoreType.DMA
    lanes = tps - 1
    return pl.pallas_call(
        functools.partial(kernel, zn, tps),
        out_shape=jax.ShapeDtypeStruct((rows, feat), bf16),
        in_specs=[vmem] * 4 + [hbm] * 4,
        out_specs=vmem,
        scratch_shapes=[
            pltpu.VMEM((width, cin), bf16),
            pltpu.VMEM((width, cin), bf16),
            pltpu.VMEM((width, fh), bf16),
            pltpu.VMEM((width, fh), bf16),
            pltpu.VMEM((own, ffw), bf16),
            pltpu.VMEM((own, ffw), bf16),
            pltpu.VMEM((tps, rows, feat), bf16),
            pltpu.VMEM((tps, 2, feat), f32),
            pltpu.VMEM((rows, width), bf16),
            pltpu.VMEM((rows, width), bf16),
            pltpu.VMEM((lanes, rows, width), bf16),
            pltpu.VMEM((2, rows, width), bf16),
            pltpu.VMEM((2 * rows, fh), bf16),
            pltpu.VMEM((n, 2 * rows, rc), bf16),
            pltpu.VMEM((lanes, per, 2 * rows, rc), bf16),
            pltpu.VMEM((per, rows, rc), bf16),
            pltpu.VMEM((per, rows, rc), bf16),
            pltpu.VMEM((rows, feat), f32),
            pltpu.VMEM((tps, rows, 128), f32),
            pltpu.VMEM((128, rows), f32),
            pltpu.VMEM((8, rows), f32),
            pltpu.VMEM((lanes, 8, rows), f32),
            pltpu.VMEM((rows, cin), f32),
            dma((6,)),
            dma((5, zn)), dma((2, zn)), dma((5, zn)), dma((5, zn)), dma((5, zn)), dma((5, zn, 2)), dma((5, zn, 2)),
            dma((lanes,)), dma((lanes,)), dma((lanes,)), dma((lanes,)),
            dma((lanes, 2)), dma((lanes, 2)), dma((2,)), dma((2,)), dma((lanes, 2)), dma((lanes, 2)),
            dma((n, 2)), dma((lanes, per, 2)), dma((per,)), dma((per,)), dma((lanes,)), dma((lanes,)),
        ],
        compiler_params=pltpu.CompilerParams(
            collective_id=0, has_side_effects=True, vmem_limit_bytes=67043328
        ),
    )(tokens, gains, pool_scale[None], gain_out[None], w_in, w_pool_out, w_ff1, w_ff2)


def solution(mesh):
    zn, tps = mesh.shape["fs"] // 4, mesh.shape["tp"]
    return jax.shard_map(
        functools.partial(local, zn, tps),
        mesh=mesh,
        in_specs=(
            P("fs", "tp"),
            P("tp"),
            P("fs", "tp"),
            P("tp"),
            P("fs", "tp"),
            P("tp"),
            P("fs", "tp"),
            P("fs", "tp"),
            P("tp"),
        ),
        out_specs=P("fs", "tp"),
        check_vma=False,
    )
```

```python
import functools
import math

import jax
import jax.numpy as jnp
from jax import lax
from jax.experimental import pallas as pl
from jax.experimental.pallas import tpu as pltpu
from jax.sharding import PartitionSpec as P

norm_eps = 1e-05
residual_alpha = 2.0**0.25
f32, bf16 = jnp.float32, jnp.bfloat16
MESH = pl.DeviceIdType.MESH
scope = jax.named_scope


def nt_dot(left, right):
    return lax.dot_general(left, right, (((1,), (1,)), ((), ())), preferred_element_type=f32)


def kernel(
    zn, tps,
    x_ref, ga_ref, gb_ref, scale_ref, gout_ref, win_ref, wpo_ref, wup_ref, wdn_ref, out_ref,
    win, wpo, wup, wdn, sup, sdn, xfull, gfull, mixed, mpart, mrecv, middle, hidden,
    part, precv, zpart, zrecv, total, moments, spread, stat, srecv, work,
    load_sem, zs_sem, zq_sem, zr_sem, ys_sem, yr_sem, ss_sem, sr_sem, xs_sem, xr_sem, gs_sem, gr_sem,
    ms_sem, mr_sem, as_sem, ar_sem, fs_sem, fr_sem, rs_sem, rr_sem, ps_sem, pr_sem, ts_sem, tr_sem,
):
    i, t = lax.axis_index("fs"), lax.axis_index("tp")
    c = lax.rem(i, 2)
    y = lax.rem(lax.div(i, 2), 2)
    z = lax.div(i, 4)
    role = lax.rem(z, 2)
    rows, feat = x_ref.shape
    cin = win_ref.shape[1]
    width = feat * tps
    own = win_ref.shape[0]
    ffw = wup_ref.shape[1]
    fh = ffw // 2
    fq = fh // 2
    n = zn * 2
    per = n // tps
    rc = own * 2
    cut = rows // 2
    ends = (0, cut, rows)
    lanes = tps - 1

    def across(j):
        other, bit = z, 1
        while bit < zn:
            if j & bit:
                other = other + bit * (1 - 2 * lax.rem(lax.div(z, bit), 2))
            bit *= 2
        return other

    order = [0]
    for j in range(1, zn // 2 + 1):
        for v in (zn // 2 + j - 1, j):
            if v not in order:
                order.append(v)
    far = order[1:]
    near = [1] + [v for j in range(2, zn, 2) for v in (j + 1, j)]

    def dev(zz, yy, cc):
        return (zz * 2 + yy) * 2 + cc

    sib = dev(z, y, 1 - c)
    opp = dev(z, 1 - y, c)
    mate = dev(across(1), y, c)
    peers = [lax.rem(t + q, tps) for q in range(1, tps)]
    mine = pl.ds(pl.multiple_of(i * own, own), own)

    WIN, WPO, UP0, UP1, DN = range(5)
    streams = [(win, 0, cin), (wpo, 0, cin), (wup, 0, fq), (wup, fq, fq), (wdn, 0, fh)]

    def block(w, zz, yy, cc):
        ref, c0, cw = streams[w]
        r0 = pl.multiple_of(dev(zz, yy, cc) * own, own)
        return ref.at[pl.ds(r0, own), pl.ds(c0, cw)]

    def remote(src, dst, send, recv, to, tt):
        return pltpu.make_async_remote_copy(
            src, dst, send, recv, device_id=(to, tt), device_id_type=MESH)

    def zsend(w, j):
        zd = across(j)
        ref, c0, cw = streams[w]
        b = block(w, z, y, c)
        if w in (WIN, WPO):
            src = b
        else:
            stage = sdn if w == DN else sup
            src = stage.at[:, pl.ds(pl.multiple_of(lax.rem(zd, 2) * fh + c0, 128), cw)]
        return remote(src, b, zs_sem.at[w, j], zr_sem.at[w, j], dev(zd, y, c), t)

    def yfwd(w, j):
        b = block(w, across(j), y, c)
        return remote(b, b, ys_sem.at[w, j], yr_sem.at[w, j], opp, t)

    def share(w, j, s):
        b = block(w, across(j), y if s == 0 else 1 - y, c)
        return remote(b, b, ss_sem.at[w, j, s], sr_sem.at[w, j, s], sib, t)

    def zsends(w, js):
        for j in js:
            zsend(w, j).start()

    def gate(me, other):
        lower = lax.rem(me, 2) == 0
        before = lax.div(other, 2) < lax.div(me, 2)
        return (lower & before) | (~lower & ~before)

    def relay(w, j):
        b = block(w, across(j), y, c)
        return remote(b, b, zq_sem.at[w, j], zr_sem.at[w, j ^ 1], mate, t)

    def spread_out(w):
        zsend(w, 1).start()
        for j in near[1:]:
            @pl.when(gate(across(j), z))
            def _():
                zsend(w, j).start()

    def own_start(w):
        yfwd(w, 0).start()
        share(w, 0, 0).start()

    def z_in(w, j):
        with scope(f"z{w}_{j}"):
            zsend(w, j).wait_recv()
        if w in (WIN, WPO) and j > 1:
            @pl.when(gate(z, across(j)))
            def _():
                relay(w, j).start()
        yfwd(w, j).start()
        share(w, j, 0).start()

    def y_in(w, j):
        with scope(f"y{w}_{j}"):
            yfwd(w, j).wait_recv()
        share(w, j, 1).start()

    def s_in(w):
        with scope(f"s{w}"):
            for j in order:
                for s in range(2):
                    share(w, j, s).wait_recv()

    def x_copy(q):
        return remote(xfull.at[t], xfull.at[t], xs_sem.at[q], xr_sem.at[q], i, peers[q])

    def g_copy(q, k):
        return remote((ga_ref, gb_ref)[k], gfull.at[k, t], gs_sem.at[q, k], gr_sem.at[q, k], i, peers[q])

    def half(h):
        return pl.ds(ends[h], ends[h + 1] - ends[h])

    def m_copy(q, h):
        return remote(mpart.at[half(h)], mrecv.at[q, half(h)], ms_sem.at[q, h], mr_sem.at[q, h], i, peers[q])

    slab = pl.ds(pl.multiple_of(t * feat, feat), feat)

    def a_copy(h):
        b = middle.at[role, half(h), slab]
        return remote(b, b, as_sem.at[h], ar_sem.at[h], mate, t)

    def f_copy(q, h):
        b = middle.at[1 - role, half(h), slab]
        return remote(b, b, fs_sem.at[q, h], fr_sem.at[q, h], i, peers[q])

    def slot(s):
        return pl.ds(pl.multiple_of(s * rows, rows), rows)

    def r_copy(g, s):
        holder, gl = lax.div(g, per), lax.rem(g, per)
        q = lax.rem(t - holder - 1 + 2 * tps, tps)
        which = (1 - role) if s == 0 else role
        return remote(
            part.at[g, slot(which)], precv.at[q, gl, slot(which)],
            rs_sem.at[g, s], rr_sem.at[q, gl, s], i, holder)

    def r_wait(q, gl, s):
        which = (1 - role) if s == 0 else role
        b = precv.at[q, gl, slot(which)]
        remote(b, b, rs_sem.at[0, s], rr_sem.at[q, gl, s], i, peers[0]).wait_recv()

    def p_copy(gl):
        return remote(zpart.at[gl], zrecv.at[gl], ps_sem.at[gl], pr_sem.at[gl], mate, t)

    def t_copy(q):
        return remote(stat, srecv.at[q], ts_sem.at[q], tr_sem.at[q], i, peers[q])

    barrier = pltpu.get_barrier_semaphore()
    for f in [dev(across(j), y, c) for j in far] + [opp, sib]:
        pl.semaphore_signal(barrier, inc=1, device_id=(f, t), device_id_type=MESH)
    for p in peers:
        pl.semaphore_signal(barrier, inc=1, device_id=(i, p), device_id_type=MESH)
    part_cols = pl.ds(pl.multiple_of(role * fh, 128), fh)
    loads = [
        pltpu.make_async_copy(win_ref, win.at[mine], load_sem.at[0]),
        pltpu.make_async_copy(wpo_ref, wpo.at[mine], load_sem.at[1]),
        pltpu.make_async_copy(wup_ref, sup, load_sem.at[2]),
        pltpu.make_async_copy(wup_ref.at[:, part_cols], wup.at[mine], load_sem.at[3]),
        pltpu.make_async_copy(wdn_ref, sdn, load_sem.at[4]),
        pltpu.make_async_copy(wdn_ref.at[:, part_cols], wdn.at[mine], load_sem.at[5]),
    ]
    x_load = pltpu.make_async_copy(x_ref, xfull.at[t], load_sem.at[6])
    x_load.start()
    for copy in loads:
        copy.start()
    with scope("begin"):
        pl.semaphore_wait(barrier, len(far) + 2 + len(peers))

    x_load.wait()
    for q in range(lanes):
        x_copy(q).start()
        for k in range(2):
            g_copy(q, k).start()
    loads[0].wait()
    own_start(WIN)
    spread_out(WIN)
    loads[1].wait()
    own_start(WPO)
    spread_out(WPO)
    loads[2].wait()
    loads[3].wait()
    gfull[0, t] = ga_ref[...]
    gfull[1, t] = gb_ref[...]
    loads[4].wait()
    loads[5].wait()

    rb = math.gcd(math.gcd(cut, rows - cut), 32)

    def blocks_of(body, lo=0, hi=rows):
        def step(r, carry):
            body(pl.ds(pl.multiple_of(lo + r * rb, rb), rb))
            return carry
        lax.fori_loop(0, (hi - lo) // rb, step, 0, unroll=2)

    def norm(pieces):
        mean = sum(jnp.sum(v, axis=1, keepdims=True) for v in pieces) / width
        pieces = [v - mean for v in pieces]
        var = sum(jnp.sum(v * v, axis=1, keepdims=True) for v in pieces) / width
        inv = lax.rsqrt(var + norm_eps)
        return [v * inv for v in pieces]

    def first_norm(rs):
        pieces = norm([xfull[r, rs, :].astype(f32) for r in range(tps)])
        for r in range(tps):
            mixed[rs, r * feat:(r + 1) * feat] = (pieces[r] * gfull[0, r]).astype(bf16)

    mids = [j for j in far if j > 1]

    def wave(w, first):
        for j in mids:
            ahead = gate(across(j), z)

            @pl.when(ahead if first else ~ahead)
            def _():
                zsend(w, j).start()

    edge = (z == 0) | (z == zn - 1)
    z_in(WIN, 1)

    @pl.when(edge)
    def _():
        z_in(WPO, 1)

    for j in near[1:]:
        z_in(WIN, j)

    @pl.when(~edge)
    def _():
        z_in(WPO, 1)

    for j in near[1:]:
        z_in(WPO, j)
    wave(UP0, True)
    y_in(WIN, 0)
    y_in(WPO, 0)
    for j in near[:-1]:
        y_in(WIN, j)
    with scope("xwait"):
        for q in range(lanes):
            x_copy(q).wait_recv()
            for k in range(2):
                g_copy(q, k).wait_recv()
    with scope("norm1"):
        blocks_of(first_norm)
    wave(UP0, False)
    zsends(UP0, [1])
    own_start(UP0)
    y_in(WIN, near[-1])
    y_in(WPO, near[0])
    s_in(WIN)

    cb = math.gcd(cin, 128)
    gw = cin * tps // 4
    with scope("pooldot"):
        pool = jnp.dot(mixed[...], win[...], preferred_element_type=f32)
        work[:, :cin] = pool.astype(bf16).astype(f32)
    for j in near[1:-1]:
        y_in(WPO, j)
    row = lax.broadcasted_iota(jnp.int32, (rows, cb), 0)
    position = (row + 1).astype(f32)
    for k in range(cin // cb):
        cs = slice(k * cb, (k + 1) * cb)
        u = work[:, cs]

        def shifted(v, steps):
            return jnp.where(row >= steps, pltpu.roll(v, steps, axis=0), 0.0)

        s2 = u + shifted(u, 1)
        s4 = s2 + shifted(s2, 2)
        s8 = s4 + shifted(s4, 4)
        s16 = s8 + shifted(s8, 8)
        channel = t * cin + k * cb + lax.broadcasted_iota(jnp.int32, (rows, cb), 1)

        def pick(a, b, e, g):
            return jnp.where(channel < gw, a, jnp.where(channel < 2 * gw, b, jnp.where(channel < 3 * gw, e, g)))

        count = jnp.minimum(position, pick(2.0, 4.0, 8.0, 16.0))
        mixed[:, cs] = ((pick(s2, s4, s8, s16) / count - u) * scale_ref[0:1, cs]).astype(bf16)

    y_in(WPO, near[-1])
    own_start(UP1)
    s_in(WPO)
    wb = math.gcd(width, 512)
    for h in range(2):
        def out_proj(k, carry):
            cs = pl.ds(pl.multiple_of(k * wb, wb), wb)
            mpart[half(h), cs] = nt_dot(mixed[half(h), :cin], wpo[cs, :]).astype(bf16)
            return carry

        with scope("outproj"):
            lax.fori_loop(0, width // wb, out_proj, 0)
        for q in range(lanes):
            m_copy(q, h).start()

    def second_norm(rs):
        pieces = []
        for r in range(tps):
            cs = slice(r * feat, (r + 1) * feat)
            mix = mpart[rs, cs].astype(f32)
            for q in range(lanes):
                mix = mix + mrecv[q, rs, cs].astype(f32)
            mix = mix.astype(bf16).astype(f32)
            pieces.append(residual_alpha * xfull[r, rs, :].astype(f32) + mix)
        pieces = norm(pieces)
        for r in range(tps):
            middle[role, rs, r * feat:(r + 1) * feat] = (pieces[r] * gfull[1, r]).astype(bf16)

    def settle(h):
        with scope("mwait"):
            for q in range(lanes):
                m_copy(q, h).wait_recv()
        with scope("norm2"):
            blocks_of(second_norm, ends[h], ends[h + 1])
        a_copy(h).start()

    wave(UP1, True)
    zsends(UP1, [1])
    z_in(UP0, 1)
    y_in(UP0, 0)
    for j in mids:
        z_in(UP0, j)
    wave(UP1, False)
    y_in(UP1, 0)
    y_in(UP0, 1)
    settle(0)
    for j in mids[:-1]:
        y_in(UP0, j)
    z_in(UP1, 1)
    y_in(UP0, mids[-1])
    for j in mids:
        z_in(UP1, j)
    own_start(DN)
    y_in(UP1, 1)
    zsends(DN, mids[:1])
    settle(1)

    @pl.when(edge)
    def _():
        zsends(DN, [1])

    hb = math.gcd(fq, 512)

    def ff1(s, lo, hi):
        def up(k, carry):
            cs = pl.ds(pl.multiple_of(lo + k * hb, hb), hb)
            act = jnp.maximum(jnp.dot(middle[s], wup[:, cs], preferred_element_type=f32), 0.0)
            hidden[slot(s), cs] = (act * act).astype(bf16)
            return carry
        with scope("ff1"):
            lax.fori_loop(0, (hi - lo) // hb, up, 0)

    def pass_on(h):
        a_back = middle.at[1 - role, half(h), slab]
        with scope("await"):
            remote(a_back, a_back, as_sem.at[h], ar_sem.at[h], mate, t).wait_recv()
        for q in range(lanes):
            f_copy(q, h).start()

    pass_on(0)
    for j in mids[:-1]:
        y_in(UP1, j)
    s_in(UP0)
    ff1(role, 0, fq)
    y_in(UP1, mids[-1])
    s_in(UP1)
    ff1(role, fq, fh)

    def group(j, s):
        return across(j) * 2 + (y if s == 0 else 1 - y)

    landed = []

    def down(j, s, kept, start=True):
        g = group(j, s)
        which = role if kept else 1 - role
        if (j, s) not in landed:
            landed.append((j, s))
            with scope(f"dshare{j}_{s}"):
                share(DN, j, s).wait_recv()
        with scope("ff2"):
            w = wdn[pl.ds(pl.multiple_of(g * rc, rc), rc), :]
            part[g, slot(which), :] = nt_dot(hidden[slot(which), :], w).astype(bf16)

        if start:
            hand(j, s, kept)

    def hand(j, s, kept):
        g = group(j, s)

        @pl.when(lax.div(g, per) != t)
        def _():
            r_copy(g, 1 if kept else 0).start()

    def both(j, s):
        down(j, s, False)
        down(j, s, True)

    def fold(j, s):
        g = group(j, s)
        gl = lax.rem(g, per)

        @pl.when(lax.div(g, per) == t)
        def _():
            with scope(f"rwait{j}_{s}"):
                for q in range(lanes):
                    r_wait(q, gl, 0)
            v = part[g, slot(1 - role), :].astype(f32)
            for q in range(lanes):
                v = v + precv[q, gl, slot(1 - role), :].astype(f32)
            zpart[gl] = v.astype(bf16)
            p_copy(gl).start()

    def residual(rs):
        base = middle[role, rs, slab]
        for gl in range(per):
            total[gl, rs, :] = residual_alpha * base[:, gl * rc:(gl + 1) * rc].astype(f32)

    def prep(j, s):
        g = group(j, s)
        gl = lax.rem(g, per)

        @pl.when(lax.div(g, per) == t)
        def _():
            with scope(f"pwait{j}_{s}"):
                for q in range(lanes):
                    r_wait(q, gl, 1)
                p_copy(gl).wait_recv()
            with scope("prep"):
                ff = part[g, slot(role), :].astype(f32)
                for q in range(lanes):
                    ff = ff + precv[q, gl, slot(role), :].astype(f32)
                total[gl] = total[gl] + (ff + zrecv[gl].astype(f32)).astype(bf16).astype(f32)

    down(0, 0, True)
    pass_on(1)

    @pl.when(~edge)
    def _():
        zsends(DN, [1])
        zsends(DN, mids[1:])

    z_in(DN, far[0])
    down(far[0], 0, True, False)
    blocks_of(residual)
    y_in(DN, 0)
    down(0, 1, True, False)

    @pl.when(~edge)
    def _():
        z_in(DN, 1)

    with scope("fwait"):
        for h in range(2):
            for q in range(lanes):
                f_copy(q, h).wait_recv()

    @pl.when(edge)
    def _():
        zsends(DN, mids[1:])
        z_in(DN, 1)

    ff1(1 - role, 0, fh)
    for ev in ((0, 0), (far[0], 0), (0, 1)):
        down(*ev, False)
    for ev in ((far[0], 0), (0, 1)):
        hand(*ev, True)
    pending = [(0, 0), (far[0], 0), (0, 1)]
    done = []
    for k in range(len(far)):
        if k and k + 1 < len(far):
            z_in(DN, far[k + 1])
        y_in(DN, far[k])
        both(far[k], 1)
        pending.append((far[k], 1))
        if k + 1 < len(far):
            both(far[k + 1], 0)
            pending.append((far[k + 1], 0))
            for ev in pending[:2 + k]:
                fold(*ev)
            done += pending[:2 + k]
            pending = pending[2 + k:]
    for ev in pending:
        fold(*ev)
    for ev in done + pending:
        prep(*ev)

    lane = lax.broadcasted_iota(jnp.int32, (rb, 128), 1)

    def gather_up(rs):
        mean = sum(jnp.sum(total[gl, rs, :], axis=1, keepdims=True) for gl in range(per)) / feat
        square = jnp.zeros((rb, 1), f32)
        for gl in range(per):
            v = total[gl, rs, :] - mean
            square = square + jnp.sum(v * v, axis=1, keepdims=True)
        moments[0, rs, :] = jnp.where(lane == 0, mean, jnp.where(lane == 1, square, 0.0))

    with scope("gather_up"):
        blocks_of(gather_up)

    def drain():
        for q in range(lanes):
            x_copy(q).wait_send()
            for k in range(2):
                g_copy(q, k).wait_send()
            for h in range(2):
                m_copy(q, h).wait_send()
                f_copy(q, h).wait_send()
        for h in range(2):
            a_copy(h).wait_send()

        def sent(g, carry):
            @pl.when(lax.div(g, per) != t)
            def _():
                r_copy(g, 0).wait_send()
                r_copy(g, 1).wait_send()
            return carry

        lax.fori_loop(0, n, sent, 0)

        def folded(gl, carry):
            p_copy(gl).wait_send()
            return carry

        lax.fori_loop(0, per, folded, 0)
        for w in range(len(streams)):
            for j in order:
                if j == 1 or (j and w not in (WIN, WPO)):
                    zsend(w, j).wait_send()
                elif j:
                    @pl.when(gate(across(j), z))
                    def _():
                        zsend(w, j).wait_send()

                    @pl.when(gate(z, across(j)))
                    def _():
                        relay(w, j).wait_send()
                yfwd(w, j).wait_send()
                share(w, j, 0).wait_send()
                share(w, j, 1).wait_send()

    stat[...] = jnp.transpose(moments[0])[0:8, :]
    for q in range(lanes):
        t_copy(q).start()
    drain()
    spread[...] = jnp.zeros_like(spread)
    for q in range(lanes):
        with scope("twait"):
            t_copy(q).wait_recv()
        spread[0:8, :] = srecv[q]
        moments[q + 1] = jnp.transpose(spread[...])

    def last_norm(rs):
        means = [moments[q, rs, 0:1] for q in range(tps)]
        mean = sum(means) / tps
        square = sum(moments[q, rs, 1:2] for q in range(tps))
        for m in means:
            square = square + feat * (m - mean) * (m - mean)
        inv = lax.rsqrt(square / width + norm_eps)
        for gl in range(per):
            cs = slice(gl * rc, (gl + 1) * rc)
            out_ref[rs, cs] = ((total[gl, rs, :] - mean) * inv * gout_ref[0:1, cs]).astype(bf16)

    with scope("norm3"):
        blocks_of(last_norm)

    for q in range(lanes):
        t_copy(q).wait_send()


def local(zn, tps, tokens, gain_mixer, w_in, pool_scale, w_pool_out, gain_mid, w_ff1, w_ff2, gain_out):
    rows, feat = tokens.shape
    own, cin = w_in.shape
    ffw = w_ff1.shape[1]
    fh = ffw // 2
    width = feat * tps
    n = zn * 2
    per = n // tps
    rc = own * 2
    vmem, hbm = pl.BlockSpec(memory_space=pltpu.VMEM), pl.BlockSpec(memory_space=pl.ANY)
    dma = pltpu.SemaphoreType.DMA
    lanes = tps - 1
    return pl.pallas_call(
        functools.partial(kernel, zn, tps),
        out_shape=jax.ShapeDtypeStruct((rows, feat), bf16),
        in_specs=[hbm] + [vmem] * 4 + [hbm] * 4,
        out_specs=vmem,
        scratch_shapes=[
            pltpu.VMEM((width, cin), bf16),
            pltpu.VMEM((width, cin), bf16),
            pltpu.VMEM((width, fh), bf16),
            pltpu.VMEM((width, fh), bf16),
            pltpu.VMEM((own, ffw), bf16),
            pltpu.VMEM((own, ffw), bf16),
            pltpu.VMEM((tps, rows, feat), bf16),
            pltpu.VMEM((2, tps, 1, feat), f32),
            pltpu.VMEM((rows, width), bf16),
            pltpu.VMEM((rows, width), bf16),
            pltpu.VMEM((lanes, rows, width), bf16),
            pltpu.VMEM((2, rows, width), bf16),
            pltpu.VMEM((2 * rows, fh), bf16),
            pltpu.VMEM((n, 2 * rows, rc), bf16),
            pltpu.VMEM((lanes, per, 2 * rows, rc), bf16),
            pltpu.VMEM((per, rows, rc), bf16),
            pltpu.VMEM((per, rows, rc), bf16),
            pltpu.VMEM((per, rows, rc), f32),
            pltpu.VMEM((tps, rows, 128), f32),
            pltpu.VMEM((128, rows), f32),
            pltpu.VMEM((8, rows), f32),
            pltpu.VMEM((lanes, 8, rows), f32),
            pltpu.VMEM((rows, cin), f32),
            dma((7,)),
            dma((5, zn)), dma((2, zn)), dma((5, zn)), dma((5, zn)), dma((5, zn)), dma((5, zn, 2)), dma((5, zn, 2)),
            dma((lanes,)), dma((lanes,)), dma((lanes, 2)), dma((lanes, 2)),
            dma((lanes, 2)), dma((lanes, 2)), dma((2,)), dma((2,)), dma((lanes, 2)), dma((lanes, 2)),
            dma((n, 2)), dma((lanes, per, 2)), dma((per,)), dma((per,)), dma((lanes,)), dma((lanes,)),
        ],
        compiler_params=pltpu.CompilerParams(
            collective_id=0, has_side_effects=True, vmem_limit_bytes=67043328
        ),
    )(tokens, gain_mixer[None], gain_mid[None], pool_scale[None], gain_out[None], w_in, w_pool_out, w_ff1, w_ff2)


def solution(mesh):
    zn, tps = mesh.shape["fs"] // 4, mesh.shape["tp"]
    return jax.shard_map(
        functools.partial(local, zn, tps),
        mesh=mesh,
        in_specs=(
            P("fs", "tp"),
            P("tp"),
            P("fs", "tp"),
            P("tp"),
            P("fs", "tp"),
            P("tp"),
            P("fs", "tp"),
            P("fs", "tp"),
            P("tp"),
        ),
        out_specs=P("fs", "tp"),
        check_vma=False,
    )
```

```python
import functools
import math

import jax
import jax.numpy as jnp
from jax import lax
from jax.experimental import pallas as pl
from jax.experimental.pallas import tpu as pltpu
from jax.sharding import PartitionSpec as P

norm_eps = 1e-05
residual_alpha = 2.0**0.25
f32, bf16 = jnp.float32, jnp.bfloat16
MESH = pl.DeviceIdType.MESH
scope = jax.named_scope


def nt_dot(left, right):
    return lax.dot_general(left, right, (((1,), (1,)), ((), ())), preferred_element_type=f32)


def kernel(
    zn, tps,
    x_ref, ga_ref, gb_ref, scale_ref, gout_ref, win_ref, wpo_ref, wup_ref, wdn_ref, out_ref,
    win, wpo, wup, wdn, sup, sdn, xfull, gfull, mixed, mpart, mrecv, middle, hidden,
    part, precv, zpart, zrecv, total, moments, spread, stat, srecv, work,
    load_sem, zs_sem, zq_sem, zr_sem, ys_sem, yr_sem, ss_sem, sr_sem, xs_sem, xr_sem, gs_sem, gr_sem,
    ms_sem, mr_sem, as_sem, ar_sem, fs_sem, fr_sem, rs_sem, rr_sem, ps_sem, pr_sem, ts_sem, tr_sem,
):
    i, t = lax.axis_index("fs"), lax.axis_index("tp")
    c = lax.rem(i, 2)
    y = lax.rem(lax.div(i, 2), 2)
    z = lax.div(i, 4)
    role = lax.rem(z, 2)
    rows, feat = x_ref.shape
    cin = win_ref.shape[1]
    width = feat * tps
    own = win_ref.shape[0]
    ffw = wup_ref.shape[1]
    spare = ffw // 16 // 256 * 256
    fh = (ffw - spare) // 2
    fq = -(-fh // 256) * 128
    n = zn * 2
    per = n // tps
    rc = own * 2
    cut = rows // 2
    ends = (0, cut, rows)
    lanes = tps - 1

    def across(j):
        other, bit = z, 1
        while bit < zn:
            if j & bit:
                other = other + bit * (1 - 2 * lax.rem(lax.div(z, bit), 2))
            bit *= 2
        return other

    order = [0]
    for j in range(1, zn // 2 + 1):
        for v in (zn // 2 + j - 1, j):
            if v not in order:
                order.append(v)
    far = order[1:]
    near = [1] + [v for j in range(2, zn, 2) for v in (j + 1, j)]

    def central(zz):
        low = lax.div(zz, max(zn // 2, 1)) == 0
        odd = lax.rem(zz, 2) == 1
        return (low & odd) | (~low & ~odd)

    taker = central(z)

    def dev(zz, yy, cc):
        return (zz * 2 + yy) * 2 + cc

    sib = dev(z, y, 1 - c)
    opp = dev(z, 1 - y, c)
    mate = dev(across(1), y, c)
    peers = [lax.rem(t + q, tps) for q in range(1, tps)]
    mine = pl.ds(pl.multiple_of(i * own, own), own)

    WIN, WPO, UP0, UPA, DN0, DNA, UPX, DNX = range(8)
    extra = (UPX, DNX)
    UP1 = (UPA, UPX) if spare else UPA
    DN = (DN0, DNA, DNX) if spare else (DN0, DNA)
    streams = [(win, 0, cin), (wpo, 0, cin), (wup, 0, fq), (wup, fq, fh - fq),
               (wdn, 0, fq), (wdn, fq, fh - fq), (wup, fh, spare), (wdn, fh, spare)]

    def block(w, zz, yy, cc):
        ref, c0, cw = streams[w]
        r0 = pl.multiple_of(dev(zz, yy, cc) * own, own)
        return ref.at[pl.ds(r0, own), pl.ds(c0, cw)]

    def remote(src, dst, send, recv, to, tt):
        return pltpu.make_async_remote_copy(
            src, dst, send, recv, device_id=(to, tt), device_id_type=MESH)

    def zsend(w, j):
        zd = across(j)
        ref, c0, cw = streams[w]
        b = block(w, z, y, c)
        if w in (WIN, WPO):
            src = b
        else:
            stage = sdn if ref is wdn else sup
            first = 2 * fh if w in extra else lax.rem(zd, 2) * fh + c0
            src = stage.at[:, pl.ds(pl.multiple_of(first, 128), cw)]
        return remote(src, b, zs_sem.at[w, j], zr_sem.at[w, j], dev(zd, y, c), t)

    def yfwd(w, j):
        b = block(w, across(j), y, c)
        return remote(b, b, ys_sem.at[w, j], yr_sem.at[w, j], opp, t)

    def share(w, j, s):
        b = block(w, across(j), y if s == 0 else 1 - y, c)
        return remote(b, b, ss_sem.at[w, j, s], sr_sem.at[w, j, s], sib, t)

    def parts(w):
        return w if isinstance(w, tuple) else (w,)

    def having(w, cond, act):
        if w in extra:
            pl.when(cond)(act)
        else:
            act()

    def zpush(ws, j):
        for w in parts(ws):
            having(w, central(across(j)), lambda: zsend(w, j).start())

    def zsends(ws, js):
        for j in js:
            zpush(ws, j)

    def gate(me, other):
        lower = lax.rem(me, 2) == 0
        before = lax.div(other, 2) < lax.div(me, 2)
        return (lower & before) | (~lower & ~before)

    def relay(w, j):
        b = block(w, across(j), y, c)
        return remote(b, b, zq_sem.at[w, j], zr_sem.at[w, j ^ 1], mate, t)

    def spread_out(w):
        zsend(w, 1).start()
        for j in near[1:]:
            @pl.when(gate(across(j), z))
            def _():
                zsend(w, j).start()

    def own_start(ws):
        for w in parts(ws):
            def act():
                yfwd(w, 0).start()
                share(w, 0, 0).start()
            having(w, taker, act)

    def z_in(ws, j):
        for w in parts(ws):
            def act():
                with scope(f"z{w}_{j}"):
                    zsend(w, j).wait_recv()
                if w in (WIN, WPO) and j > 1:
                    @pl.when(gate(z, across(j)))
                    def _():
                        relay(w, j).start()
                yfwd(w, j).start()
                share(w, j, 0).start()
            having(w, taker, act)

    def y_in(ws, j):
        for w in parts(ws):
            def act():
                with scope(f"y{w}_{j}"):
                    yfwd(w, j).wait_recv()
                share(w, j, 1).start()
            having(w, taker, act)

    def s_wait(ws, j, s):
        for w in parts(ws):
            having(w, taker, lambda: share(w, j, s).wait_recv())

    def s_in(ws):
        with scope(f"s{parts(ws)[0]}"):
            for j in order:
                for s in range(2):
                    s_wait(ws, j, s)

    head = rows * 3 // 4

    def x_copy(q, k):
        b = xfull.at[t, pl.ds(k * head, (rows - head) if k else head)]
        return remote(b, b, xs_sem.at[q, k], xr_sem.at[q, k], i, peers[q])

    def g_copy(q, k):
        return remote((ga_ref, gb_ref)[k], gfull.at[k, t], gs_sem.at[q, k], gr_sem.at[q, k], i, peers[q])

    def half(h):
        return pl.ds(ends[h], ends[h + 1] - ends[h])

    def m_copy(q, h):
        return remote(mpart.at[half(h)], mrecv.at[q, half(h)], ms_sem.at[q, h], mr_sem.at[q, h], i, peers[q])

    slab = pl.ds(pl.multiple_of(t * feat, feat), feat)

    def a_copy(h):
        b = middle.at[role, half(h), slab]
        return remote(b, b, as_sem.at[h], ar_sem.at[h], mate, t)

    def f_copy(q, h):
        b = middle.at[1 - role, half(h), slab]
        return remote(b, b, fs_sem.at[q, h], fr_sem.at[q, h], i, peers[q])

    def slot(s):
        return pl.ds(pl.multiple_of(s * rows, rows), rows)

    def r_copy(g, s):
        holder, gl = lax.div(g, per), lax.rem(g, per)
        q = lax.rem(t - holder - 1 + 2 * tps, tps)
        which = (1 - role) if s == 0 else role
        return remote(
            part.at[g, slot(which)], precv.at[q, gl, slot(which)],
            rs_sem.at[g, s], rr_sem.at[q, gl, s], i, holder)

    def r_wait(q, gl, s):
        which = (1 - role) if s == 0 else role
        b = precv.at[q, gl, slot(which)]
        remote(b, b, rs_sem.at[0, s], rr_sem.at[q, gl, s], i, peers[0]).wait_recv()

    def p_copy(gl):
        return remote(zpart.at[gl], zrecv.at[gl], ps_sem.at[gl], pr_sem.at[gl], mate, t)

    def t_copy(q):
        return remote(stat, srecv.at[q], ts_sem.at[q], tr_sem.at[q], i, peers[q])

    barrier = pltpu.get_barrier_semaphore()
    for f in [dev(across(j), y, c) for j in far] + [opp, sib]:
        pl.semaphore_signal(barrier, inc=1, device_id=(f, t), device_id_type=MESH)
    for p in peers:
        pl.semaphore_signal(barrier, inc=1, device_id=(i, p), device_id_type=MESH)
    part_cols = pl.ds(pl.multiple_of(role * fh, 128), fh)
    loads = [
        pltpu.make_async_copy(win_ref, win.at[mine], load_sem.at[0]),
        pltpu.make_async_copy(wpo_ref, wpo.at[mine], load_sem.at[1]),
        pltpu.make_async_copy(wup_ref, sup, load_sem.at[2]),
        pltpu.make_async_copy(wup_ref.at[:, part_cols], wup.at[mine, pl.ds(0, fh)], load_sem.at[3]),
        pltpu.make_async_copy(wdn_ref, sdn, load_sem.at[4]),
        pltpu.make_async_copy(wdn_ref.at[:, part_cols], wdn.at[mine, pl.ds(0, fh)], load_sem.at[5]),
    ]
    if spare:
        for k, (src, dst) in enumerate(((wup_ref, wup), (wdn_ref, wdn))):
            loads.append(pltpu.make_async_copy(
                src.at[:, pl.ds(2 * fh, spare)], dst.at[mine, pl.ds(fh, spare)], load_sem.at[7 + k]))
    x_load = pltpu.make_async_copy(x_ref, xfull.at[t], load_sem.at[6])
    x_load.start()
    for copy in loads:
        copy.start()
    with scope("begin"):
        pl.semaphore_wait(barrier, len(far) + 2 + len(peers))

    x_load.wait()
    for q in range(lanes):
        for k in range(2):
            g_copy(q, k).start()
            x_copy(q, k).start()
    loads[0].wait()
    own_start(WIN)
    spread_out(WIN)
    loads[1].wait()
    own_start(WPO)
    spread_out(WPO)
    loads[2].wait()
    loads[3].wait()
    gfull[0, t] = ga_ref[...]
    gfull[1, t] = gb_ref[...]
    for copy in loads[4:]:
        copy.wait()

    rb = math.gcd(math.gcd(cut, rows - cut), 32)

    def blocks_of(body, lo=0, hi=rows):
        def step(r, carry):
            body(pl.ds(pl.multiple_of(lo + r * rb, rb), rb))
            return carry
        lax.fori_loop(0, (hi - lo) // rb, step, 0, unroll=2)

    def norm(pieces):
        mean = sum(jnp.sum(v, axis=1, keepdims=True) for v in pieces) / width
        pieces = [v - mean for v in pieces]
        var = sum(jnp.sum(v * v, axis=1, keepdims=True) for v in pieces) / width
        inv = lax.rsqrt(var + norm_eps)
        return [v * inv for v in pieces]

    def first_norm(rs):
        pieces = norm([xfull[r, rs, :].astype(f32) for r in range(tps)])
        for r in range(tps):
            mixed[rs, r * feat:(r + 1) * feat] = (pieces[r] * gfull[0, r]).astype(bf16)

    mids = [j for j in far if j > 1]

    def wave(w, first):
        for j in mids:
            ahead = gate(across(j), z)

            @pl.when(ahead if first else ~ahead)
            def _():
                zpush(w, j)

    edge = (z == 0) | (z == zn - 1)
    z_in(WIN, 1)

    @pl.when(edge)
    def _():
        z_in(WPO, 1)

    for j in near[1:]:
        z_in(WIN, j)

    @pl.when(~edge)
    def _():
        z_in(WPO, 1)

    for j in near[1:]:
        z_in(WPO, j)
    wave(UP0, True)
    y_in(WIN, 0)
    y_in(WPO, 0)
    for j in near[:-1]:
        y_in(WIN, j)
    for k in range(2):
        with scope("xwait"):
            for q in range(lanes):
                if k == 0:
                    for v in range(2):
                        g_copy(q, v).wait_recv()
                x_copy(q, k).wait_recv()
        with scope("norm1"):
            blocks_of(first_norm, k * head, rows if k else head)
        if k == 0:
            wave(UP0, False)
            zsends(UP0, [1])
            own_start(UP0)
    y_in(WIN, near[-1])
    y_in(WPO, near[0])
    s_in(WIN)

    cb = math.gcd(cin, 128)
    gw = cin * tps // 4
    with scope("pooldot"):
        pool = jnp.dot(mixed[...], win[...], preferred_element_type=f32)
        work[:, :cin] = pool.astype(bf16).astype(f32)
    for j in near[1:-1]:
        y_in(WPO, j)
    row = lax.broadcasted_iota(jnp.int32, (rows, cb), 0)
    position = (row + 1).astype(f32)
    for k in range(cin // cb):
        cs = slice(k * cb, (k + 1) * cb)
        u = work[:, cs]

        def shifted(v, steps):
            return jnp.where(row >= steps, pltpu.roll(v, steps, axis=0), 0.0)

        s2 = u + shifted(u, 1)
        s4 = s2 + shifted(s2, 2)
        s8 = s4 + shifted(s4, 4)
        s16 = s8 + shifted(s8, 8)
        channel = t * cin + k * cb + lax.broadcasted_iota(jnp.int32, (rows, cb), 1)

        def pick(a, b, e, g):
            return jnp.where(channel < gw, a, jnp.where(channel < 2 * gw, b, jnp.where(channel < 3 * gw, e, g)))

        count = jnp.minimum(position, pick(2.0, 4.0, 8.0, 16.0))
        mixed[:, cs] = ((pick(s2, s4, s8, s16) / count - u) * scale_ref[0:1, cs]).astype(bf16)

    y_in(WPO, near[-1])
    own_start(UP1)
    s_in(WPO)
    wb = math.gcd(width, 512)
    for h in range(2):
        def out_proj(k, carry):
            cs = pl.ds(pl.multiple_of(k * wb, wb), wb)
            mpart[half(h), cs] = nt_dot(mixed[half(h), :cin], wpo[cs, :]).astype(bf16)
            return carry

        with scope("outproj"):
            lax.fori_loop(0, width // wb, out_proj, 0)
        for q in range(lanes):
            m_copy(q, h).start()

    def second_norm(rs):
        pieces = []
        for r in range(tps):
            cs = slice(r * feat, (r + 1) * feat)
            mix = mpart[rs, cs].astype(f32)
            for q in range(lanes):
                mix = mix + mrecv[q, rs, cs].astype(f32)
            mix = mix.astype(bf16).astype(f32)
            pieces.append(residual_alpha * xfull[r, rs, :].astype(f32) + mix)
        pieces = norm(pieces)
        for r in range(tps):
            middle[role, rs, r * feat:(r + 1) * feat] = (pieces[r] * gfull[1, r]).astype(bf16)

    def settle(h):
        with scope("mwait"):
            for q in range(lanes):
                m_copy(q, h).wait_recv()
        with scope("norm2"):
            blocks_of(second_norm, ends[h], ends[h + 1])
        a_copy(h).start()

    wave(UP1, True)
    zsends(UP1, [1])
    z_in(UP0, 1)
    y_in(UP0, 0)
    for j in mids:
        z_in(UP0, j)
    wave(UP1, False)
    y_in(UP1, 0)
    y_in(UP0, 1)
    settle(0)
    for j in mids[:-1]:
        y_in(UP0, j)
    z_in(UP1, 1)
    y_in(UP0, mids[-1])
    for j in mids:
        z_in(UP1, j)
    own_start(DN)
    y_in(UP1, 1)
    zsends(DN, mids[:1])
    settle(1)

    @pl.when(edge)
    def _():
        zsends(DN, [1])

    hb = min(fq, 512)

    def ff1(s, lo, hi):
        def up(c0, cw):
            cs = pl.ds(c0, cw)
            act = jnp.maximum(jnp.dot(middle[s], wup[:, cs], preferred_element_type=f32), 0.0)
            hidden[slot(s), cs] = (act * act).astype(bf16)

        def step(k, carry):
            up(pl.multiple_of(lo + k * hb, 128), hb)
            return carry

        with scope("ff1"):
            whole = (hi - lo) // hb
            lax.fori_loop(0, whole, step, 0)
            if (hi - lo) % hb:
                up(lo + whole * hb, (hi - lo) % hb)
            if spare and hi == fh:
                @pl.when(taker)
                def _():
                    up(fh, spare)

    def pass_on(h):
        a_back = middle.at[1 - role, half(h), slab]
        with scope("await"):
            remote(a_back, a_back, as_sem.at[h], ar_sem.at[h], mate, t).wait_recv()
        for q in range(lanes):
            f_copy(q, h).start()

    pass_on(0)
    for j in mids[:-1]:
        y_in(UP1, j)
    s_in(UP0)
    ff1(role, 0, fq)
    y_in(UP1, mids[-1])
    s_in(UP1)
    ff1(role, fq, fh)

    def group(j, s):
        return across(j) * 2 + (y if s == 0 else 1 - y)

    landed = []

    def down(j, s, kept):
        g = group(j, s)
        which = role if kept else 1 - role
        if (j, s) not in landed:
            landed.append((j, s))
            with scope(f"dshare{j}_{s}"):
                s_wait(DN, j, s)
        with scope("ff2"):
            rhs = pl.ds(pl.multiple_of(g * rc, rc), rc)

            def product(depth):
                part[g, slot(which), :] = nt_dot(hidden[slot(which), :depth], wdn[rhs, :depth]).astype(bf16)

            if spare:
                pl.when(taker)(lambda: product(fh + spare))
                pl.when(~taker)(lambda: product(fh))
            else:
                product(fh)

        @pl.when(lax.div(g, per) != t)
        def _():
            r_copy(g, 1 if kept else 0).start()

    def both(j, s):
        down(j, s, False)
        down(j, s, True)

    def fold(j, s):
        g = group(j, s)
        gl = lax.rem(g, per)

        @pl.when(lax.div(g, per) == t)
        def _():
            with scope(f"rwait{j}_{s}"):
                for q in range(lanes):
                    r_wait(q, gl, 0)
            v = part[g, slot(1 - role), :].astype(f32)
            for q in range(lanes):
                v = v + precv[q, gl, slot(1 - role), :].astype(f32)
            zpart[gl] = v.astype(bf16)
            p_copy(gl).start()

    def residual(rs):
        base = middle[role, rs, slab]
        for gl in range(per):
            total[gl, rs, :] = residual_alpha * base[:, gl * rc:(gl + 1) * rc].astype(f32)

    def prep(j, s):
        g = group(j, s)
        gl = lax.rem(g, per)

        @pl.when(lax.div(g, per) == t)
        def _():
            with scope(f"pwait{j}_{s}"):
                for q in range(lanes):
                    r_wait(q, gl, 1)
                p_copy(gl).wait_recv()
            with scope("prep"):
                ff = part[g, slot(role), :].astype(f32)
                for q in range(lanes):
                    ff = ff + precv[q, gl, slot(role), :].astype(f32)
                total[gl] = total[gl] + (ff + zrecv[gl].astype(f32)).astype(bf16).astype(f32)

    down(0, 0, True)
    pass_on(1)

    @pl.when(~edge)
    def _():
        zsends(DN, [1])
        zsends(DN, mids[1:])

    z_in(DN, far[0])
    down(far[0], 0, True)
    blocks_of(residual)
    y_in(DN, 0)
    down(0, 1, True)

    @pl.when(~edge)
    def _():
        z_in(DN, 1)

    with scope("fwait"):
        for h in range(2):
            for q in range(lanes):
                f_copy(q, h).wait_recv()

    @pl.when(edge)
    def _():
        zsends(DN, mids[1:])
        z_in(DN, 1)

    ff1(1 - role, 0, fh)
    for ev in ((0, 0), (far[0], 0), (0, 1)):
        down(*ev, False)
    pending = [(0, 0), (far[0], 0), (0, 1)]
    done = []
    for k in range(len(far)):
        if k and k + 1 < len(far):
            z_in(DN, far[k + 1])
        y_in(DN, far[k])
        late = [(far[k + 1], 0)] if k + 1 < len(far) else []
        for ev in late + [(far[k], 1)]:
            both(*ev)
            pending.append(ev)
        if late:
            for ev in pending[:2 + k]:
                fold(*ev)
            done += pending[:2 + k]
            pending = pending[2 + k:]
    for ev in pending:
        fold(*ev)
    for ev in done + pending:
        prep(*ev)

    lane = lax.broadcasted_iota(jnp.int32, (rb, 128), 1)

    def gather_up(rs):
        mean = sum(jnp.sum(total[gl, rs, :], axis=1, keepdims=True) for gl in range(per)) / feat
        square = jnp.zeros((rb, 1), f32)
        for gl in range(per):
            v = total[gl, rs, :] - mean
            square = square + jnp.sum(v * v, axis=1, keepdims=True)
        moments[0, rs, :] = jnp.where(lane == 0, mean, jnp.where(lane == 1, square, 0.0))

    with scope("gather_up"):
        blocks_of(gather_up)

    def drain():
        for q in range(lanes):
            for k in range(2):
                x_copy(q, k).wait_send()
                g_copy(q, k).wait_send()
            for h in range(2):
                m_copy(q, h).wait_send()
                f_copy(q, h).wait_send()
        for h in range(2):
            a_copy(h).wait_send()

        def sent(g, carry):
            @pl.when(lax.div(g, per) != t)
            def _():
                r_copy(g, 0).wait_send()
                r_copy(g, 1).wait_send()
            return carry

        lax.fori_loop(0, n, sent, 0)

        def folded(gl, carry):
            p_copy(gl).wait_send()
            return carry

        lax.fori_loop(0, per, folded, 0)
        for w in range(len(streams) if spare else len(streams) - 2):
            for j in order:
                if j == 1 or (j and w not in (WIN, WPO)):
                    having(w, central(across(j)), lambda: zsend(w, j).wait_send())
                elif j:
                    @pl.when(gate(across(j), z))
                    def _():
                        zsend(w, j).wait_send()

                    @pl.when(gate(z, across(j)))
                    def _():
                        relay(w, j).wait_send()

                def rest():
                    yfwd(w, j).wait_send()
                    share(w, j, 0).wait_send()
                    share(w, j, 1).wait_send()
                having(w, taker, rest)

    stat[...] = jnp.transpose(moments[0])[0:8, :]
    for q in range(lanes):
        t_copy(q).start()
    drain()
    spread[...] = jnp.zeros_like(spread)
    for q in range(lanes):
        with scope("twait"):
            t_copy(q).wait_recv()
        spread[0:8, :] = srecv[q]
        moments[q + 1] = jnp.transpose(spread[...])

    def last_norm(rs):
        means = [moments[q, rs, 0:1] for q in range(tps)]
        mean = sum(means) / tps
        square = sum(moments[q, rs, 1:2] for q in range(tps))
        for m in means:
            square = square + feat * (m - mean) * (m - mean)
        inv = lax.rsqrt(square / width + norm_eps)
        for gl in range(per):
            cs = slice(gl * rc, (gl + 1) * rc)
            out_ref[rs, cs] = ((total[gl, rs, :] - mean) * inv * gout_ref[0:1, cs]).astype(bf16)

    with scope("norm3"):
        blocks_of(last_norm)

    for q in range(lanes):
        t_copy(q).wait_send()


def local(zn, tps, tokens, gain_mixer, w_in, pool_scale, w_pool_out, gain_mid, w_ff1, w_ff2, gain_out):
    rows, feat = tokens.shape
    own, cin = w_in.shape
    ffw = w_ff1.shape[1]
    fh = (ffw + ffw // 16 // 256 * 256) // 2
    width = feat * tps
    n = zn * 2
    per = n // tps
    rc = own * 2
    vmem, hbm = pl.BlockSpec(memory_space=pltpu.VMEM), pl.BlockSpec(memory_space=pl.ANY)
    dma = pltpu.SemaphoreType.DMA
    lanes = tps - 1
    return pl.pallas_call(
        functools.partial(kernel, zn, tps),
        out_shape=jax.ShapeDtypeStruct((rows, feat), bf16),
        in_specs=[hbm] + [vmem] * 4 + [hbm] * 4,
        out_specs=vmem,
        scratch_shapes=[
            pltpu.VMEM((width, cin), bf16),
            pltpu.VMEM((width, cin), bf16),
            pltpu.VMEM((width, fh), bf16),
            pltpu.VMEM((width, fh), bf16),
            pltpu.VMEM((own, ffw), bf16),
            pltpu.VMEM((own, ffw), bf16),
            pltpu.VMEM((tps, rows, feat), bf16),
            pltpu.VMEM((2, tps, 1, feat), f32),
            pltpu.VMEM((rows, width), bf16),
            pltpu.VMEM((rows, width), bf16),
            pltpu.VMEM((lanes, rows, width), bf16),
            pltpu.VMEM((2, rows, width), bf16),
            pltpu.VMEM((2 * rows, fh), bf16),
            pltpu.VMEM((n, 2 * rows, rc), bf16),
            pltpu.VMEM((lanes, per, 2 * rows, rc), bf16),
            pltpu.VMEM((per, rows, rc), bf16),
            pltpu.VMEM((per, rows, rc), bf16),
            pltpu.VMEM((per, rows, rc), f32),
            pltpu.VMEM((tps, rows, 128), f32),
            pltpu.VMEM((128, rows), f32),
            pltpu.VMEM((8, rows), f32),
            pltpu.VMEM((lanes, 8, rows), f32),
            pltpu.VMEM((rows, cin), f32),
            dma((9,)),
            dma((8, zn)), dma((2, zn)), dma((8, zn)), dma((8, zn)), dma((8, zn)), dma((8, zn, 2)), dma((8, zn, 2)),
            dma((lanes, 2)), dma((lanes, 2)), dma((lanes, 2)), dma((lanes, 2)),
            dma((lanes, 2)), dma((lanes, 2)), dma((2,)), dma((2,)), dma((lanes, 2)), dma((lanes, 2)),
            dma((n, 2)), dma((lanes, per, 2)), dma((per,)), dma((per,)), dma((lanes,)), dma((lanes,)),
        ],
        compiler_params=pltpu.CompilerParams(
            collective_id=0, has_side_effects=True, vmem_limit_bytes=67043328
        ),
    )(tokens, gain_mixer[None], gain_mid[None], pool_scale[None], gain_out[None], w_in, w_pool_out, w_ff1, w_ff2)


def solution(mesh):
    zn, tps = mesh.shape["fs"] // 4, mesh.shape["tp"]
    return jax.shard_map(
        functools.partial(local, zn, tps),
        mesh=mesh,
        in_specs=(
            P("fs", "tp"),
            P("tp"),
            P("fs", "tp"),
            P("tp"),
            P("fs", "tp"),
            P("tp"),
            P("fs", "tp"),
            P("fs", "tp"),
            P("tp"),
        ),
        out_specs=P("fs", "tp"),
        check_vma=False,
    )
```

```python
import functools
import math

import jax
import jax.numpy as jnp
from jax import lax
from jax.experimental import pallas as pl
from jax.experimental.pallas import tpu as pltpu
from jax.sharding import PartitionSpec as P

norm_eps = 1e-05
residual_alpha = 2.0**0.25
f32, bf16 = jnp.float32, jnp.bfloat16
MESH = pl.DeviceIdType.MESH
scope = jax.named_scope


def nt_dot(left, right):
    return lax.dot_general(left, right, (((1,), (1,)), ((), ())), preferred_element_type=f32)


def kernel(
    zn, tps,
    x_ref, ga_ref, gb_ref, scale_ref, gout_ref, win_ref, wpo_ref, wup_ref, wdn_ref, out_ref,
    win, wpo, wup, wdn, sup, sdn, xfull, gfull, mixed, mpart, mrecv, middle, hidden,
    part, precv, zpart, zrecv, total, moments, spread, stat, srecv, work,
    load_sem, zs_sem, zq_sem, zr_sem, ys_sem, yr_sem, ss_sem, sr_sem, dr_sem, xs_sem, xr_sem, gs_sem, gr_sem,
    ms_sem, mr_sem, as_sem, ar_sem, fs_sem, fr_sem, rs_sem, rr_sem, ps_sem, pr_sem, ts_sem, tr_sem,
):
    i, t = lax.axis_index("fs"), lax.axis_index("tp")
    c = lax.rem(i, 2)
    y = lax.rem(lax.div(i, 2), 2)
    z = lax.div(i, 4)
    role = lax.rem(z, 2)
    rows, feat = x_ref.shape
    cin = win_ref.shape[1]
    width = feat * tps
    own = win_ref.shape[0]
    ffw = wup_ref.shape[1]
    spare = ffw // 16 // 256 * 256
    fh = (ffw - spare) // 2
    fq = -(-fh // 256) * 128
    n = zn * 2
    per = n // tps
    rc = own * 2
    cut = rows // 2
    ends = (0, cut, rows)
    lanes = tps - 1

    def across(j):
        other, bit = z, 1
        while bit < zn:
            if j & bit:
                other = other + bit * (1 - 2 * lax.rem(lax.div(z, bit), 2))
            bit *= 2
        return other

    order = [0]
    for j in range(1, zn // 2 + 1):
        for v in (zn // 2 + j - 1, j):
            if v not in order:
                order.append(v)
    far = order[1:]
    near = [1] + [v for j in range(2, zn, 2) for v in (j + 1, j)]

    def central(zz):
        low = lax.div(zz, max(zn // 2, 1)) == 0
        odd = lax.rem(zz, 2) == 1
        return (low & odd) | (~low & ~odd)

    taker = central(z)

    def dev(zz, yy, cc):
        return (zz * 2 + yy) * 2 + cc

    sib = dev(z, y, 1 - c)
    opp = dev(z, 1 - y, c)
    mate = dev(across(1), y, c)
    peers = [lax.rem(t + q, tps) for q in range(1, tps)]
    mine = pl.ds(pl.multiple_of(i * own, own), own)

    WIN, WPO, UP0, UPA, DN0, DNA, UPX, DNX = range(8)
    extra = (UPX, DNX)
    UP1 = (UPA, UPX) if spare else UPA
    DN = (DN0, DNA, DNX) if spare else (DN0, DNA)
    streams = [(win, 0, cin), (wpo, 0, cin), (wup, 0, fq), (wup, fq, fh - fq),
               (wdn, 0, fq), (wdn, fq, fh - fq), (wup, fh, spare), (wdn, fh, spare)]

    def block(w, zz, yy, cc):
        ref, c0, cw = streams[w]
        r0 = pl.multiple_of(dev(zz, yy, cc) * own, own)
        return ref.at[pl.ds(r0, own), pl.ds(c0, cw)]

    def remote(src, dst, send, recv, to, tt):
        return pltpu.make_async_remote_copy(
            src, dst, send, recv, device_id=(to, tt), device_id_type=MESH)

    def zsend(w, j):
        zd = across(j)
        ref, c0, cw = streams[w]
        b = block(w, z, y, c)
        if w in (WIN, WPO):
            src = b
        else:
            stage = sdn if ref is wdn else sup
            first = 2 * fh if w in extra else lax.rem(zd, 2) * fh + c0
            src = stage.at[:, pl.ds(pl.multiple_of(first, 128), cw)]
        return remote(src, b, zs_sem.at[w], zr_sem.at[w, j], dev(zd, y, c), t)

    def yfwd(w, j):
        b = block(w, across(j), y, c)
        return remote(b, b, ys_sem.at[w], yr_sem.at[w, j], opp, t)

    def share(w, j, s):
        b = block(w, across(j), y if s == 0 else 1 - y, c)
        return remote(b, b, ss_sem.at[w], dr_sem.at[j, s] if w in DN else sr_sem.at[w], sib, t)

    def parts(w):
        return w if isinstance(w, tuple) else (w,)

    def having(w, cond, act):
        if w in extra:
            pl.when(cond)(act)
        else:
            act()

    def zpush(ws, j):
        for w in parts(ws):
            having(w, central(across(j)), lambda: zsend(w, j).start())

    def zsends(ws, js):
        for j in js:
            zpush(ws, j)

    def gate(me, other):
        lower = lax.rem(me, 2) == 0
        before = lax.div(other, 2) < lax.div(me, 2)
        return (lower & before) | (~lower & ~before)

    def relay(w, j):
        b = block(w, across(j), y, c)
        return remote(b, b, zq_sem.at[w, j], zr_sem.at[w, j ^ 1], mate, t)

    def spread_out(w):
        zsend(w, 1).start()
        for j in near[1:]:
            @pl.when(gate(across(j), z))
            def _():
                zsend(w, j).start()

    def own_start(ws):
        for w in parts(ws):
            def act():
                yfwd(w, 0).start()
                share(w, 0, 0).start()
            having(w, taker, act)

    def z_in(ws, j):
        for w in parts(ws):
            def act():
                with scope(f"z{w}_{j}"):
                    zsend(w, j).wait_recv()
                if w in (WIN, WPO) and j > 1:
                    @pl.when(gate(z, across(j)))
                    def _():
                        relay(w, j).start()
                yfwd(w, j).start()
                share(w, j, 0).start()
            having(w, taker, act)

    def y_in(ws, j):
        for w in parts(ws):
            def act():
                with scope(f"y{w}_{j}"):
                    yfwd(w, j).wait_recv()
                share(w, j, 1).start()
            having(w, taker, act)

    def stretch(w, count):
        ref, c0, cw = streams[w]
        return ref.at[pl.ds(0, count * own), pl.ds(c0, cw)]

    def d_wait(j, s):
        def act(depth):
            b = wdn.at[pl.ds(0, own), pl.ds(0, depth)]
            remote(b, b, ss_sem.at[DN0], dr_sem.at[j, s], sib, t).wait_recv()

        if spare:
            pl.when(taker)(lambda: act(fh + spare))
            pl.when(~taker)(lambda: act(fh))
        else:
            act(fh)

    def s_in(ws):
        with scope(f"s{parts(ws)[0]}"):
            for w in parts(ws):
                b = stretch(w, 2 * zn)
                having(w, taker, lambda: remote(b, b, ss_sem.at[w], sr_sem.at[w], sib, t).wait_recv())

    head = rows * 3 // 4

    def x_copy(q, k):
        b = xfull.at[t, pl.ds(k * head, (rows - head) if k else head)]
        return remote(b, b, xs_sem.at[q, k], xr_sem.at[q, k], i, peers[q])

    def g_copy(q, k):
        return remote((ga_ref, gb_ref)[k], gfull.at[k, t], gs_sem.at[q, k], gr_sem.at[q, k], i, peers[q])

    def half(h):
        return pl.ds(ends[h], ends[h + 1] - ends[h])

    def m_copy(q, h):
        return remote(mpart.at[half(h)], mrecv.at[q, half(h)], ms_sem.at[q, h], mr_sem.at[q, h], i, peers[q])

    slab = pl.ds(pl.multiple_of(t * feat, feat), feat)

    def a_copy(h):
        b = middle.at[role, half(h), slab]
        return remote(b, b, as_sem.at[h], ar_sem.at[h], mate, t)

    def f_copy(q, h):
        b = middle.at[1 - role, half(h), slab]
        return remote(b, b, fs_sem.at[q, h], fr_sem.at[q, h], i, peers[q])

    def slot(s):
        return pl.ds(pl.multiple_of(s * rows, rows), rows)

    def r_copy(g, s):
        holder, gl = lax.div(g, per), lax.rem(g, per)
        q = lax.rem(t - holder - 1 + 2 * tps, tps)
        which = (1 - role) if s == 0 else role
        return remote(
            part.at[g, slot(which)], precv.at[q, gl, slot(which)],
            rs_sem.at[g, s], rr_sem.at[q, gl, s], i, holder)

    def r_wait(q, gl, s):
        which = (1 - role) if s == 0 else role
        b = precv.at[q, gl, slot(which)]
        remote(b, b, rs_sem.at[0, s], rr_sem.at[q, gl, s], i, peers[0]).wait_recv()

    def p_copy(gl):
        return remote(zpart.at[gl], zrecv.at[gl], ps_sem.at[gl], pr_sem.at[gl], mate, t)

    def t_copy(q):
        return remote(stat, srecv.at[q], ts_sem.at[q], tr_sem.at[q], i, peers[q])

    barrier = pltpu.get_barrier_semaphore()
    for f in [dev(across(j), y, c) for j in far] + [opp, sib]:
        pl.semaphore_signal(barrier, inc=1, device_id=(f, t), device_id_type=MESH)
    for p in peers:
        pl.semaphore_signal(barrier, inc=1, device_id=(i, p), device_id_type=MESH)
    part_cols = pl.ds(pl.multiple_of(role * fh, 128), fh)
    loads = [
        pltpu.make_async_copy(win_ref, win.at[mine], load_sem.at[0]),
        pltpu.make_async_copy(wpo_ref, wpo.at[mine], load_sem.at[1]),
        pltpu.make_async_copy(wup_ref, sup, load_sem.at[2]),
        pltpu.make_async_copy(wup_ref.at[:, part_cols], wup.at[mine, pl.ds(0, fh)], load_sem.at[3]),
        pltpu.make_async_copy(wdn_ref, sdn, load_sem.at[4]),
        pltpu.make_async_copy(wdn_ref.at[:, part_cols], wdn.at[mine, pl.ds(0, fh)], load_sem.at[5]),
    ]
    if spare:
        for k, (src, dst) in enumerate(((wup_ref, wup), (wdn_ref, wdn))):
            loads.append(pltpu.make_async_copy(
                src.at[:, pl.ds(2 * fh, spare)], dst.at[mine, pl.ds(fh, spare)], load_sem.at[7 + k]))
    x_load = pltpu.make_async_copy(x_ref, xfull.at[t], load_sem.at[6])
    x_load.start()
    for copy in loads:
        copy.start()
    with scope("begin"):
        pl.semaphore_wait(barrier, len(far) + 2 + len(peers))

    x_load.wait()
    for q in range(lanes):
        for k in range(2):
            g_copy(q, k).start()
            x_copy(q, k).start()
    loads[0].wait()
    own_start(WIN)
    spread_out(WIN)
    loads[1].wait()
    own_start(WPO)
    spread_out(WPO)
    loads[2].wait()
    loads[3].wait()
    gfull[0, t] = ga_ref[...]
    gfull[1, t] = gb_ref[...]
    for copy in loads[4:]:
        copy.wait()

    rb = math.gcd(math.gcd(cut, rows - cut), 32)

    def blocks_of(body, lo=0, hi=rows):
        def step(r, carry):
            body(pl.ds(pl.multiple_of(lo + r * rb, rb), rb))
            return carry
        lax.fori_loop(0, (hi - lo) // rb, step, 0, unroll=2)

    def norm(pieces):
        mean = sum(jnp.sum(v, axis=1, keepdims=True) for v in pieces) / width
        pieces = [v - mean for v in pieces]
        var = sum(jnp.sum(v * v, axis=1, keepdims=True) for v in pieces) / width
        inv = lax.rsqrt(var + norm_eps)
        return [v * inv for v in pieces]

    def first_norm(rs):
        pieces = norm([xfull[r, rs, :].astype(f32) for r in range(tps)])
        for r in range(tps):
            mixed[rs, r * feat:(r + 1) * feat] = (pieces[r] * gfull[0, r]).astype(bf16)

    mids = [j for j in far if j > 1]

    def wave(w, first):
        for j in mids:
            ahead = gate(across(j), z)

            @pl.when(ahead if first else ~ahead)
            def _():
                zpush(w, j)

    edge = (z == 0) | (z == zn - 1)
    z_in(WIN, 1)

    @pl.when(edge)
    def _():
        z_in(WPO, 1)

    for j in near[1:]:
        z_in(WIN, j)

    @pl.when(~edge)
    def _():
        z_in(WPO, 1)

    for j in near[1:]:
        z_in(WPO, j)
    wave(UP0, True)
    y_in(WIN, 0)
    y_in(WPO, 0)
    for j in near[:-1]:
        y_in(WIN, j)
    for k in range(2):
        with scope("xwait"):
            for q in range(lanes):
                if k == 0:
                    for v in range(2):
                        g_copy(q, v).wait_recv()
                x_copy(q, k).wait_recv()
        with scope("norm1"):
            blocks_of(first_norm, k * head, rows if k else head)
        if k == 0:
            wave(UP0, False)
            zsends(UP0, [1])
            own_start(UP0)
    y_in(WIN, near[-1])
    y_in(WPO, near[0])
    s_in(WIN)

    cb = math.gcd(cin, 128)
    gw = cin * tps // 4
    with scope("pooldot"):
        pool = jnp.dot(mixed[...], win[...], preferred_element_type=f32)
        work[:, :cin] = pool.astype(bf16).astype(f32)
    for j in near[1:-1]:
        y_in(WPO, j)
    row = lax.broadcasted_iota(jnp.int32, (rows, cb), 0)
    position = (row + 1).astype(f32)
    for k in range(cin // cb):
        cs = slice(k * cb, (k + 1) * cb)
        u = work[:, cs]

        def shifted(v, steps):
            return jnp.where(row >= steps, pltpu.roll(v, steps, axis=0), 0.0)

        s2 = u + shifted(u, 1)
        s4 = s2 + shifted(s2, 2)
        s8 = s4 + shifted(s4, 4)
        s16 = s8 + shifted(s8, 8)
        channel = t * cin + k * cb + lax.broadcasted_iota(jnp.int32, (rows, cb), 1)

        def pick(a, b, e, g):
            return jnp.where(channel < gw, a, jnp.where(channel < 2 * gw, b, jnp.where(channel < 3 * gw, e, g)))

        count = jnp.minimum(position, pick(2.0, 4.0, 8.0, 16.0))
        mixed[:, cs] = ((pick(s2, s4, s8, s16) / count - u) * scale_ref[0:1, cs]).astype(bf16)

    y_in(WPO, near[-1])
    own_start(UP1)
    s_in(WPO)
    wb = math.gcd(width, 512)
    for h in range(2):
        def out_proj(k, carry):
            cs = pl.ds(pl.multiple_of(k * wb, wb), wb)
            mpart[half(h), cs] = nt_dot(mixed[half(h), :cin], wpo[cs, :]).astype(bf16)
            return carry

        with scope("outproj"):
            lax.fori_loop(0, width // wb, out_proj, 0)
        for q in range(lanes):
            m_copy(q, h).start()

    def second_norm(rs):
        pieces = []
        for r in range(tps):
            cs = slice(r * feat, (r + 1) * feat)
            mix = mpart[rs, cs].astype(f32)
            for q in range(lanes):
                mix = mix + mrecv[q, rs, cs].astype(f32)
            mix = mix.astype(bf16).astype(f32)
            pieces.append(residual_alpha * xfull[r, rs, :].astype(f32) + mix)
        pieces = norm(pieces)
        for r in range(tps):
            middle[role, rs, r * feat:(r + 1) * feat] = (pieces[r] * gfull[1, r]).astype(bf16)

    def settle(h):
        with scope("mwait"):
            for q in range(lanes):
                m_copy(q, h).wait_recv()
        with scope("norm2"):
            blocks_of(second_norm, ends[h], ends[h + 1])
        a_copy(h).start()

    wave(UP1, True)
    zsends(UP1, [1])
    z_in(UP0, 1)
    y_in(UP0, 0)
    for j in mids:
        z_in(UP0, j)
    wave(UP1, False)
    y_in(UP1, 0)
    y_in(UP0, 1)
    settle(0)
    for j in mids[:-1]:
        y_in(UP0, j)
    z_in(UP1, 1)
    y_in(UP0, mids[-1])
    for j in mids:
        z_in(UP1, j)
    own_start(DN)
    y_in(UP1, 1)
    zsends(DN, mids[:1])
    settle(1)

    @pl.when(edge)
    def _():
        zsends(DN, [1])

    hb = min(fq, 512)

    def ff1(s, lo, hi, h=None):
        if h is None:
            r0, count = 0, rows
        else:
            r0, count = ends[h], ends[h + 1] - ends[h]

        def up(c0, cw):
            cs = pl.ds(c0, cw)
            act = jnp.dot(middle[s, pl.ds(r0, count), :], wup[:, cs], preferred_element_type=f32)
            act = jnp.maximum(act, 0.0)
            to = pl.ds(pl.multiple_of(s * rows + r0, 16), count)
            hidden[to, cs] = (act * act).astype(bf16)

        def step(k, carry):
            up(pl.multiple_of(lo + k * hb, 128), hb)
            return carry

        with scope("ff1"):
            whole = (hi - lo) // hb
            lax.fori_loop(0, whole, step, 0)
            if (hi - lo) % hb:
                up(lo + whole * hb, (hi - lo) % hb)
            if spare and hi == fh:
                @pl.when(taker)
                def _():
                    up(fh, spare)

    def pass_on(h):
        a_back = middle.at[1 - role, half(h), slab]
        with scope("await"):
            remote(a_back, a_back, as_sem.at[h], ar_sem.at[h], mate, t).wait_recv()
        for q in range(lanes):
            f_copy(q, h).start()

    pass_on(0)
    for j in mids[:-1]:
        y_in(UP1, j)
    s_in(UP0)
    ff1(role, 0, fq)
    y_in(UP1, mids[-1])
    s_in(UP1)
    ff1(role, fq, fh)

    def group(j, s):
        return across(j) * 2 + (y if s == 0 else 1 - y)

    landed = []

    def down(j, s, kept):
        g = group(j, s)
        which = role if kept else 1 - role
        if (j, s) not in landed:
            landed.append((j, s))
            with scope(f"dshare{j}_{s}"):
                d_wait(j, s)
        with scope("ff2"):
            rhs = pl.ds(pl.multiple_of(g * rc, rc), rc)

            def product(depth):
                part[g, slot(which), :] = nt_dot(hidden[slot(which), :depth], wdn[rhs, :depth]).astype(bf16)

            if spare:
                pl.when(taker)(lambda: product(fh + spare))
                pl.when(~taker)(lambda: product(fh))
            else:
                product(fh)

        @pl.when(lax.div(g, per) != t)
        def _():
            r_copy(g, 1 if kept else 0).start()

    def both(j, s):
        down(j, s, False)
        down(j, s, True)

    def fold(j, s):
        g = group(j, s)
        gl = lax.rem(g, per)

        @pl.when(lax.div(g, per) == t)
        def _():
            with scope(f"rwait{j}_{s}"):
                for q in range(lanes):
                    r_wait(q, gl, 0)
            v = part[g, slot(1 - role), :].astype(f32)
            for q in range(lanes):
                v = v + precv[q, gl, slot(1 - role), :].astype(f32)
            zpart[gl] = v.astype(bf16)
            p_copy(gl).start()

    def residual(rs):
        base = middle[role, rs, slab]
        for gl in range(per):
            total[gl, rs, :] = residual_alpha * base[:, gl * rc:(gl + 1) * rc].astype(f32)

    def prep(j, s):
        g = group(j, s)
        gl = lax.rem(g, per)

        @pl.when(lax.div(g, per) == t)
        def _():
            with scope(f"pwait{j}_{s}"):
                for q in range(lanes):
                    r_wait(q, gl, 1)
                p_copy(gl).wait_recv()
            with scope("prep"):
                ff = part[g, slot(role), :].astype(f32)
                for q in range(lanes):
                    ff = ff + precv[q, gl, slot(role), :].astype(f32)
                total[gl] = total[gl] + (ff + zrecv[gl].astype(f32)).astype(bf16).astype(f32)

    down(0, 0, True)
    pass_on(1)

    @pl.when(~edge)
    def _():
        zsends(DN, [1])
        zsends(DN, mids[1:])

    z_in(DN, far[0])
    down(far[0], 0, True)
    blocks_of(residual)
    y_in(DN, 0)
    down(0, 1, True)

    def f_wait(h):
        with scope("fwait"):
            for q in range(lanes):
                f_copy(q, h).wait_recv()

    f_wait(0)
    ff1(1 - role, 0, fh, 0)

    @pl.when(~edge)
    def _():
        z_in(DN, 1)

    f_wait(1)

    @pl.when(edge)
    def _():
        zsends(DN, mids[1:])
        z_in(DN, 1)

    ff1(1 - role, 0, fh, 1)
    for ev in ((far[0], 0), (0, 0), (0, 1)):
        down(*ev, False)
    pending = [(0, 0), (far[0], 0), (0, 1)]
    done = []
    for k in range(len(far)):
        if k and k + 1 < len(far):
            z_in(DN, far[k + 1])
        y_in(DN, far[k])
        late = [(far[k + 1], 0)] if k + 1 < len(far) else []
        for ev in late + [(far[k], 1)]:
            both(*ev)
            pending.append(ev)
        if late:
            for ev in pending[:2 + k]:
                fold(*ev)
            done += pending[:2 + k]
            pending = pending[2 + k:]
    for ev in pending:
        fold(*ev)
    for ev in done + pending:
        prep(*ev)

    lane = lax.broadcasted_iota(jnp.int32, (rb, 128), 1)

    def gather_up(rs):
        mean = sum(jnp.sum(total[gl, rs, :], axis=1, keepdims=True) for gl in range(per)) / feat
        square = jnp.zeros((rb, 1), f32)
        for gl in range(per):
            v = total[gl, rs, :] - mean
            square = square + jnp.sum(v * v, axis=1, keepdims=True)
        moments[0, rs, :] = jnp.where(lane == 0, mean, jnp.where(lane == 1, square, 0.0))

    with scope("gather_up"):
        blocks_of(gather_up)

    def drain():
        for q in range(lanes):
            for k in range(2):
                x_copy(q, k).wait_send()
                g_copy(q, k).wait_send()
            for h in range(2):
                m_copy(q, h).wait_send()
                f_copy(q, h).wait_send()
        for h in range(2):
            a_copy(h).wait_send()

        def sent(g, carry):
            @pl.when(lax.div(g, per) != t)
            def _():
                r_copy(g, 0).wait_send()
                r_copy(g, 1).wait_send()
            return carry

        lax.fori_loop(0, n, sent, 0)

        def folded(gl, carry):
            p_copy(gl).wait_send()
            return carry

        lax.fori_loop(0, per, folded, 0)
        def gone(sem, w, count):
            if count:
                b = stretch(w, count)
                remote(b, b, sem.at[w], zr_sem.at[w, 0], opp, t).wait_send()

        for w in range(len(streams) if spare else len(streams) - 2):
            if w in extra:
                pl.when(taker)(lambda: gone(zs_sem, w, zn // 2 - 1))
                pl.when(~taker)(lambda: gone(zs_sem, w, zn // 2))
            else:
                gone(zs_sem, w, zn // 2 if w in (WIN, WPO) else zn - 1)

            def rest():
                gone(ys_sem, w, zn)
                gone(ss_sem, w, 2 * zn)
            having(w, taker, rest)
            if w in (WIN, WPO):
                for j in near[1:]:
                    @pl.when(gate(z, across(j)))
                    def _():
                        relay(w, j).wait_send()

    stat[...] = jnp.transpose(moments[0])[0:8, :]
    for q in range(lanes):
        t_copy(q).start()
    drain()
    spread[...] = jnp.zeros_like(spread)
    for q in range(lanes):
        with scope("twait"):
            t_copy(q).wait_recv()
        spread[0:8, :] = srecv[q]
        moments[q + 1] = jnp.transpose(spread[...])

    def last_norm(rs):
        means = [moments[q, rs, 0:1] for q in range(tps)]
        mean = sum(means) / tps
        square = sum(moments[q, rs, 1:2] for q in range(tps))
        for m in means:
            square = square + feat * (m - mean) * (m - mean)
        inv = lax.rsqrt(square / width + norm_eps)
        for gl in range(per):
            cs = slice(gl * rc, (gl + 1) * rc)
            out_ref[rs, cs] = ((total[gl, rs, :] - mean) * inv * gout_ref[0:1, cs]).astype(bf16)

    with scope("norm3"):
        blocks_of(last_norm)

    for q in range(lanes):
        t_copy(q).wait_send()


def local(zn, tps, tokens, gain_mixer, w_in, pool_scale, w_pool_out, gain_mid, w_ff1, w_ff2, gain_out):
    rows, feat = tokens.shape
    own, cin = w_in.shape
    ffw = w_ff1.shape[1]
    fh = (ffw + ffw // 16 // 256 * 256) // 2
    width = feat * tps
    n = zn * 2
    per = n // tps
    rc = own * 2
    vmem, hbm = pl.BlockSpec(memory_space=pltpu.VMEM), pl.BlockSpec(memory_space=pl.ANY)
    dma = pltpu.SemaphoreType.DMA
    lanes = tps - 1
    return pl.pallas_call(
        functools.partial(kernel, zn, tps),
        out_shape=jax.ShapeDtypeStruct((rows, feat), bf16),
        in_specs=[hbm] + [vmem] * 4 + [hbm] * 4,
        out_specs=vmem,
        scratch_shapes=[
            pltpu.VMEM((width, cin), bf16),
            pltpu.VMEM((width, cin), bf16),
            pltpu.VMEM((width, fh), bf16),
            pltpu.VMEM((width, fh), bf16),
            pltpu.VMEM((own, ffw), bf16),
            pltpu.VMEM((own, ffw), bf16),
            pltpu.VMEM((tps, rows, feat), bf16),
            pltpu.VMEM((2, tps, 1, feat), f32),
            pltpu.VMEM((rows, width), bf16),
            pltpu.VMEM((rows, width), bf16),
            pltpu.VMEM((lanes, rows, width), bf16),
            pltpu.VMEM((2, rows, width), bf16),
            pltpu.VMEM((2 * rows, fh), bf16),
            pltpu.VMEM((n, 2 * rows, rc), bf16),
            pltpu.VMEM((lanes, per, 2 * rows, rc), bf16),
            pltpu.VMEM((per, rows, rc), bf16),
            pltpu.VMEM((per, rows, rc), bf16),
            pltpu.VMEM((per, rows, rc), f32),
            pltpu.VMEM((tps, rows, 128), f32),
            pltpu.VMEM((128, rows), f32),
            pltpu.VMEM((8, rows), f32),
            pltpu.VMEM((lanes, 8, rows), f32),
            pltpu.VMEM((rows, cin), f32),
            dma((9,)),
            dma((8,)), dma((2, zn)), dma((8, zn)), dma((8,)), dma((8, zn)), dma((8,)), dma((8,)), dma((zn, 2)),
            dma((lanes, 2)), dma((lanes, 2)), dma((lanes, 2)), dma((lanes, 2)),
            dma((lanes, 2)), dma((lanes, 2)), dma((2,)), dma((2,)), dma((lanes, 2)), dma((lanes, 2)),
            dma((n, 2)), dma((lanes, per, 2)), dma((per,)), dma((per,)), dma((lanes,)), dma((lanes,)),
        ],
        compiler_params=pltpu.CompilerParams(
            collective_id=0, has_side_effects=True, vmem_limit_bytes=67043328
        ),
    )(tokens, gain_mixer[None], gain_mid[None], pool_scale[None], gain_out[None], w_in, w_pool_out, w_ff1, w_ff2)


def solution(mesh):
    zn, tps = mesh.shape["fs"] // 4, mesh.shape["tp"]
    return jax.shard_map(
        functools.partial(local, zn, tps),
        mesh=mesh,
        in_specs=(
            P("fs", "tp"),
            P("tp"),
            P("fs", "tp"),
            P("tp"),
            P("fs", "tp"),
            P("tp"),
            P("fs", "tp"),
            P("fs", "tp"),
            P("tp"),
        ),
        out_specs=P("fs", "tp"),
        check_vma=False,
    )
```

```python
import functools
import math

import jax
import jax.numpy as jnp
from jax import lax
from jax.experimental import pallas as pl
from jax.experimental.pallas import tpu as pltpu
from jax.sharding import PartitionSpec as P

norm_eps = 1e-05
residual_alpha = 2.0**0.25
f32, bf16 = jnp.float32, jnp.bfloat16
MESH = pl.DeviceIdType.MESH
scope = jax.named_scope


def nt_dot(left, right):
    return lax.dot_general(left, right, (((1,), (1,)), ((), ())), preferred_element_type=f32)


def kernel(
    zn, tps,
    x_ref, ga_ref, gb_ref, scale_ref, gout_ref, win_ref, wpo_ref, wup_ref, wdn_ref, out_ref,
    win, wpo, wup, wdn, sup, sdn, xfull, gfull, mixed, mpart, mrecv, middle, hidden,
    part, precv, zpart, zrecv, total, moments, spread, stat, srecv, work,
    load_sem, zs_sem, zq_sem, zr_sem, ys_sem, yr_sem, ss_sem, sr_sem, dr_sem, xs_sem, xr_sem, gs_sem, gr_sem,
    ms_sem, mr_sem, as_sem, ar_sem, fs_sem, fr_sem, rs_sem, rr_sem, ps_sem, pr_sem, ts_sem, tr_sem,
):
    i, t = lax.axis_index("fs"), lax.axis_index("tp")
    c = lax.rem(i, 2)
    y = lax.rem(lax.div(i, 2), 2)
    z = lax.div(i, 4)
    role = lax.rem(z, 2)
    rows, feat = x_ref.shape
    cin = win_ref.shape[1]
    width = feat * tps
    own = win_ref.shape[0]
    ffw = wup_ref.shape[1]
    spare = ffw // 16 // 256 * 256
    fh = (ffw - spare) // 2
    fq = -(-fh // 256) * 128
    n = zn * 2
    per = n // tps
    rc = own * 2
    cut = rows // 2
    ends = (0, cut, rows)
    lanes = tps - 1

    def across(j):
        other, bit = z, 1
        while bit < zn:
            if j & bit:
                other = other + bit * (1 - 2 * lax.rem(lax.div(z, bit), 2))
            bit *= 2
        return other

    order = [0]
    for j in range(1, zn // 2 + 1):
        for v in (zn // 2 + j - 1, j):
            if v not in order:
                order.append(v)
    far = order[1:]
    near = [1] + [v for j in range(2, zn, 2) for v in (j + 1, j)]

    def central(zz):
        low = lax.div(zz, max(zn // 2, 1)) == 0
        odd = lax.rem(zz, 2) == 1
        return (low & odd) | (~low & ~odd)

    taker = central(z)

    def dev(zz, yy, cc):
        return (zz * 2 + yy) * 2 + cc

    sib = dev(z, y, 1 - c)
    opp = dev(z, 1 - y, c)
    mate = dev(across(1), y, c)
    peers = [lax.rem(t + q, tps) for q in range(1, tps)]
    mine = pl.ds(pl.multiple_of(i * own, own), own)

    WIN, WPO, UP0, UPA, DN0, DNA, UPX, DNX = range(8)
    extra = (UPX, DNX)
    UP1 = (UPA, UPX) if spare else UPA
    DN = (DN0, DNA, DNX) if spare else (DN0, DNA)
    streams = [(win, 0, cin), (wpo, 0, cin), (wup, 0, fq), (wup, fq, fh - fq),
               (wdn, 0, fq), (wdn, fq, fh - fq), (wup, fh, spare), (wdn, fh, spare)]

    def block(w, zz, yy, cc):
        ref, c0, cw = streams[w]
        r0 = pl.multiple_of(dev(zz, yy, cc) * own, own)
        return ref.at[pl.ds(r0, own), pl.ds(c0, cw)]

    def remote(src, dst, send, recv, to, tt):
        return pltpu.make_async_remote_copy(
            src, dst, send, recv, device_id=(to, tt), device_id_type=MESH)

    def zsend(w, j):
        zd = across(j)
        ref, c0, cw = streams[w]
        b = block(w, z, y, c)
        if w in (WIN, WPO):
            src = b
        else:
            stage = sdn if ref is wdn else sup
            first = 2 * fh if w in extra else lax.rem(zd, 2) * fh + c0
            src = stage.at[:, pl.ds(pl.multiple_of(first, 128), cw)]
        return remote(src, b, zs_sem.at[w], zr_sem.at[w, j], dev(zd, y, c), t)

    def yfwd(w, j):
        b = block(w, across(j), y, c)
        return remote(b, b, ys_sem.at[w], yr_sem.at[w, j], opp, t)

    def share(w, j, s):
        b = block(w, across(j), y if s == 0 else 1 - y, c)
        return remote(b, b, ss_sem.at[w], dr_sem.at[j, s] if w in DN else sr_sem.at[w], sib, t)

    def parts(w):
        return w if isinstance(w, tuple) else (w,)

    def having(w, cond, act):
        if w in extra:
            pl.when(cond)(act)
        else:
            act()

    def zpush(ws, j):
        for w in parts(ws):
            having(w, central(across(j)), lambda: zsend(w, j).start())

    def zsends(ws, js):
        for j in js:
            zpush(ws, j)

    def gate(me, other):
        lower = lax.rem(me, 2) == 0
        before = lax.div(other, 2) < lax.div(me, 2)
        return (lower & before) | (~lower & ~before)

    def relay(w, j):
        b = block(w, across(j), y, c)
        return remote(b, b, zq_sem.at[w, j], zr_sem.at[w, j ^ 1], mate, t)

    def spread_out(w):
        zsend(w, 1).start()
        for j in near[1:]:
            @pl.when(gate(across(j), z))
            def _():
                zsend(w, j).start()

    def own_start(ws):
        for w in parts(ws):
            def act():
                yfwd(w, 0).start()
                share(w, 0, 0).start()
            having(w, taker, act)

    def z_in(ws, j):
        for w in parts(ws):
            def act():
                with scope(f"z{w}_{j}"):
                    zsend(w, j).wait_recv()
                if w in (WIN, WPO) and j > 1:
                    @pl.when(gate(z, across(j)))
                    def _():
                        relay(w, j).start()
                yfwd(w, j).start()
                share(w, j, 0).start()
            having(w, taker, act)

    def y_in(ws, j):
        for w in parts(ws):
            def act():
                with scope(f"y{w}_{j}"):
                    yfwd(w, j).wait_recv()
                share(w, j, 1).start()
            having(w, taker, act)

    def stretch(w, count):
        ref, c0, cw = streams[w]
        return ref.at[pl.ds(0, count * own), pl.ds(c0, cw)]

    def d_wait(j, s):
        def act(depth):
            b = wdn.at[pl.ds(0, own), pl.ds(0, depth)]
            remote(b, b, ss_sem.at[DN0], dr_sem.at[j, s], sib, t).wait_recv()

        if spare:
            pl.when(taker)(lambda: act(fh + spare))
            pl.when(~taker)(lambda: act(fh))
        else:
            act(fh)

    def s_in(ws):
        with scope(f"s{parts(ws)[0]}"):
            for w in parts(ws):
                b = stretch(w, 2 * zn)
                having(w, taker, lambda: remote(b, b, ss_sem.at[w], sr_sem.at[w], sib, t).wait_recv())

    head = rows * 3 // 4

    def x_copy(q, k):
        b = xfull.at[t, pl.ds(k * head, (rows - head) if k else head)]
        return remote(b, b, xs_sem.at[q, k], xr_sem.at[q, k], i, peers[q])

    def g_copy(q, k):
        return remote((ga_ref, gb_ref)[k], gfull.at[k, t], gs_sem.at[q, k], gr_sem.at[q, k], i, peers[q])

    def half(h):
        return pl.ds(ends[h], ends[h + 1] - ends[h])

    def m_copy(q, h):
        return remote(mpart.at[half(h)], mrecv.at[q, half(h)], ms_sem.at[q, h], mr_sem.at[q, h], i, peers[q])

    slab = pl.ds(pl.multiple_of(t * feat, feat), feat)

    def a_copy(h):
        b = middle.at[role, half(h), slab]
        return remote(b, b, as_sem.at[h], ar_sem.at[h], mate, t)

    def f_copy(q, h):
        b = middle.at[1 - role, half(h), slab]
        return remote(b, b, fs_sem.at[q, h], fr_sem.at[q, h], i, peers[q])

    def slot(s):
        return pl.ds(pl.multiple_of(s * rows, rows), rows)

    def r_copy(g, s):
        holder, gl = lax.div(g, per), lax.rem(g, per)
        q = lax.rem(t - holder - 1 + 2 * tps, tps)
        which = (1 - role) if s == 0 else role
        return remote(
            part.at[g, slot(which)], precv.at[q, gl, slot(which)],
            rs_sem.at[g, s], rr_sem.at[q, gl, s], i, holder)

    def r_wait(q, gl, s):
        which = (1 - role) if s == 0 else role
        b = precv.at[q, gl, slot(which)]
        remote(b, b, rs_sem.at[0, s], rr_sem.at[q, gl, s], i, peers[0]).wait_recv()

    def p_copy(gl):
        return remote(zpart.at[gl], zrecv.at[gl], ps_sem.at[gl], pr_sem.at[gl], mate, t)

    def t_copy(q):
        return remote(stat, srecv.at[q], ts_sem.at[q], tr_sem.at[q], i, peers[q])

    barrier = pltpu.get_barrier_semaphore()
    for f in [dev(across(j), y, c) for j in far] + [opp, sib]:
        pl.semaphore_signal(barrier, inc=1, device_id=(f, t), device_id_type=MESH)
    for p in peers:
        pl.semaphore_signal(barrier, inc=1, device_id=(i, p), device_id_type=MESH)
    part_cols = pl.ds(pl.multiple_of(role * fh, 128), fh)
    loads = [
        pltpu.make_async_copy(win_ref, win.at[mine], load_sem.at[0]),
        pltpu.make_async_copy(wpo_ref, wpo.at[mine], load_sem.at[1]),
        pltpu.make_async_copy(wup_ref, sup, load_sem.at[2]),
        pltpu.make_async_copy(wup_ref.at[:, part_cols], wup.at[mine, pl.ds(0, fh)], load_sem.at[3]),
        pltpu.make_async_copy(wdn_ref, sdn, load_sem.at[4]),
        pltpu.make_async_copy(wdn_ref.at[:, part_cols], wdn.at[mine, pl.ds(0, fh)], load_sem.at[5]),
    ]
    if spare:
        for k, (src, dst) in enumerate(((wup_ref, wup), (wdn_ref, wdn))):
            loads.append(pltpu.make_async_copy(
                src.at[:, pl.ds(2 * fh, spare)], dst.at[mine, pl.ds(fh, spare)], load_sem.at[7 + k]))
    x_load = pltpu.make_async_copy(x_ref, xfull.at[t], load_sem.at[6])
    x_load.start()
    for copy in loads:
        copy.start()
    with scope("begin"):
        pl.semaphore_wait(barrier, len(far) + 2 + len(peers))

    x_load.wait()
    for q in range(lanes):
        for k in range(2):
            g_copy(q, k).start()
            x_copy(q, k).start()
    loads[0].wait()
    own_start(WIN)
    spread_out(WIN)
    loads[1].wait()
    own_start(WPO)
    spread_out(WPO)
    loads[2].wait()
    loads[3].wait()
    gfull[0, t] = ga_ref[...]
    gfull[1, t] = gb_ref[...]
    for copy in loads[4:]:
        copy.wait()

    rb = math.gcd(math.gcd(cut, rows - cut), 32)

    def blocks_of(body, lo=0, hi=rows):
        def step(r, carry):
            body(pl.ds(pl.multiple_of(lo + r * rb, rb), rb))
            return carry
        lax.fori_loop(0, (hi - lo) // rb, step, 0, unroll=2)

    def norm(pieces):
        mean = sum(jnp.sum(v, axis=1, keepdims=True) for v in pieces) / width
        pieces = [v - mean for v in pieces]
        var = sum(jnp.sum(v * v, axis=1, keepdims=True) for v in pieces) / width
        inv = lax.rsqrt(var + norm_eps)
        return [v * inv for v in pieces]

    def first_norm(rs):
        pieces = norm([xfull[r, rs, :].astype(f32) for r in range(tps)])
        for r in range(tps):
            mixed[rs, r * feat:(r + 1) * feat] = (pieces[r] * gfull[0, r]).astype(bf16)

    mids = [j for j in far if j > 1]

    def wave(w, first):
        for j in mids:
            ahead = gate(across(j), z)

            @pl.when(ahead if first else ~ahead)
            def _():
                zpush(w, j)

    edge = (z == 0) | (z == zn - 1)
    z_in(WIN, 1)

    @pl.when(edge)
    def _():
        z_in(WPO, 1)

    for j in near[1:]:
        z_in(WIN, j)

    @pl.when(~edge)
    def _():
        z_in(WPO, 1)

    for j in near[1:]:
        z_in(WPO, j)
    wave(UP0, True)
    y_in(WIN, 0)
    y_in(WPO, 0)
    for j in near[:-1]:
        y_in(WIN, j)
    for k in range(2):
        with scope("xwait"):
            for q in range(lanes):
                if k == 0:
                    for v in range(2):
                        g_copy(q, v).wait_recv()
                x_copy(q, k).wait_recv()
        with scope("norm1"):
            blocks_of(first_norm, k * head, rows if k else head)
        if k == 0:
            wave(UP0, False)
            zsends(UP0, [1])
            own_start(UP0)
    y_in(WIN, near[-1])
    y_in(WPO, near[0])
    s_in(WIN)

    cb = math.gcd(cin, 128)
    gw = cin * tps // 4
    with scope("pooldot"):
        pool = jnp.dot(mixed[...], win[...], preferred_element_type=f32)
        work[:, :cin] = pool.astype(bf16).astype(f32)
    for j in near[1:-1]:
        y_in(WPO, j)
    row = lax.broadcasted_iota(jnp.int32, (rows, cb), 0)
    position = (row + 1).astype(f32)
    for k in range(cin // cb):
        cs = slice(k * cb, (k + 1) * cb)
        u = work[:, cs]

        def shifted(v, steps):
            return jnp.where(row >= steps, pltpu.roll(v, steps, axis=0), 0.0)

        s2 = u + shifted(u, 1)
        s4 = s2 + shifted(s2, 2)
        s8 = s4 + shifted(s4, 4)
        s16 = s8 + shifted(s8, 8)
        channel = t * cin + k * cb + lax.broadcasted_iota(jnp.int32, (rows, cb), 1)

        def pick(a, b, e, g):
            return jnp.where(channel < gw, a, jnp.where(channel < 2 * gw, b, jnp.where(channel < 3 * gw, e, g)))

        count = jnp.minimum(position, pick(2.0, 4.0, 8.0, 16.0))
        mixed[:, cs] = ((pick(s2, s4, s8, s16) / count - u) * scale_ref[0:1, cs]).astype(bf16)

    y_in(WPO, near[-1])
    own_start(UP1)
    s_in(WPO)
    wb = math.gcd(width, 512)
    for h in range(2):
        def out_proj(k, carry):
            cs = pl.ds(pl.multiple_of(k * wb, wb), wb)
            mpart[half(h), cs] = nt_dot(mixed[half(h), :cin], wpo[cs, :]).astype(bf16)
            return carry

        with scope("outproj"):
            lax.fori_loop(0, width // wb, out_proj, 0)
        for q in range(lanes):
            m_copy(q, h).start()

    def second_norm(rs):
        pieces = []
        for r in range(tps):
            cs = slice(r * feat, (r + 1) * feat)
            mix = mpart[rs, cs].astype(f32)
            for q in range(lanes):
                mix = mix + mrecv[q, rs, cs].astype(f32)
            mix = mix.astype(bf16).astype(f32)
            pieces.append(residual_alpha * xfull[r, rs, :].astype(f32) + mix)
        pieces = norm(pieces)
        for r in range(tps):
            middle[role, rs, r * feat:(r + 1) * feat] = (pieces[r] * gfull[1, r]).astype(bf16)

    def settle(h):
        with scope("mwait"):
            for q in range(lanes):
                m_copy(q, h).wait_recv()
        with scope("norm2"):
            blocks_of(second_norm, ends[h], ends[h + 1])
        a_copy(h).start()

    wave(UP1, True)
    zsends(UP1, [1])
    z_in(UP0, 1)
    y_in(UP0, 0)
    for j in mids:
        z_in(UP0, j)
    wave(UP1, False)
    y_in(UP1, 0)
    y_in(UP0, 1)
    settle(0)
    for j in mids[:-1]:
        y_in(UP0, j)
    z_in(UP1, 1)
    y_in(UP0, mids[-1])
    for j in mids:
        z_in(UP1, j)
    own_start(DN)
    y_in(UP1, 1)
    zsends(DN, mids[:1])
    settle(1)

    @pl.when(edge)
    def _():
        zsends(DN, [1])

    hb = min(fq, 512)

    def ff1(s, lo, hi, h=None):
        if h is None:
            r0, count = 0, rows
        else:
            r0, count = ends[h], ends[h + 1] - ends[h]

        def up(c0, cw):
            cs = pl.ds(c0, cw)
            act = jnp.dot(middle[s, pl.ds(r0, count), :], wup[:, cs], preferred_element_type=f32)
            act = jnp.maximum(act, 0.0)
            to = pl.ds(pl.multiple_of(s * rows + r0, 16), count)
            hidden[to, cs] = (act * act).astype(bf16)

        def step(k, carry):
            up(pl.multiple_of(lo + k * hb, 128), hb)
            return carry

        with scope("ff1"):
            whole = (hi - lo) // hb
            lax.fori_loop(0, whole, step, 0)
            if (hi - lo) % hb:
                up(lo + whole * hb, (hi - lo) % hb)
            if spare and hi == fh:
                @pl.when(taker)
                def _():
                    up(fh, spare)

    def pass_on(h):
        a_back = middle.at[1 - role, half(h), slab]
        with scope("await"):
            remote(a_back, a_back, as_sem.at[h], ar_sem.at[h], mate, t).wait_recv()
        for q in range(lanes):
            f_copy(q, h).start()

    pass_on(0)
    for j in mids[:-1]:
        y_in(UP1, j)
    s_in(UP0)
    ff1(role, 0, fq)
    y_in(UP1, mids[-1])
    s_in(UP1)
    ff1(role, fq, fh)

    def group(j, s):
        return across(j) * 2 + (y if s == 0 else 1 - y)

    landed = []

    def down(j, s, kept):
        g = group(j, s)
        which = role if kept else 1 - role
        if (j, s) not in landed:
            landed.append((j, s))
            with scope(f"dshare{j}_{s}"):
                d_wait(j, s)
        with scope("ff2"):
            rhs = pl.ds(pl.multiple_of(g * rc, rc), rc)

            def product(depth):
                part[g, slot(which), :] = nt_dot(hidden[slot(which), :depth], wdn[rhs, :depth]).astype(bf16)

            if spare:
                pl.when(taker)(lambda: product(fh + spare))
                pl.when(~taker)(lambda: product(fh))
            else:
                product(fh)

        @pl.when(lax.div(g, per) != t)
        def _():
            r_copy(g, 1 if kept else 0).start()

    def both(j, s):
        down(j, s, False)
        down(j, s, True)

    def fold(j, s):
        g = group(j, s)
        gl = lax.rem(g, per)

        @pl.when(lax.div(g, per) == t)
        def _():
            with scope(f"rwait{j}_{s}"):
                for q in range(lanes):
                    r_wait(q, gl, 0)
            v = part[g, slot(1 - role), :].astype(f32)
            for q in range(lanes):
                v = v + precv[q, gl, slot(1 - role), :].astype(f32)
            zpart[gl] = v.astype(bf16)
            p_copy(gl).start()

    def residual(rs):
        base = middle[role, rs, slab]
        for gl in range(per):
            total[gl, rs, :] = residual_alpha * base[:, gl * rc:(gl + 1) * rc].astype(f32)

    def prep(j, s):
        g = group(j, s)
        gl = lax.rem(g, per)

        @pl.when(lax.div(g, per) == t)
        def _():
            with scope(f"pwait{j}_{s}"):
                for q in range(lanes):
                    r_wait(q, gl, 1)
                p_copy(gl).wait_recv()
            with scope("prep"):
                ff = part[g, slot(role), :].astype(f32)
                for q in range(lanes):
                    ff = ff + precv[q, gl, slot(role), :].astype(f32)
                total[gl] = total[gl] + (ff + zrecv[gl].astype(f32)).astype(bf16).astype(f32)

    down(0, 0, True)

    @pl.when(edge)
    def _():
        z_in(DN, far[0])

    pass_on(1)

    @pl.when(~edge)
    def _():
        zsends(DN, [1])
        zsends(DN, mids[1:])


    @pl.when(~edge)
    def _():
        z_in(DN, far[0])

    down(far[0], 0, True)
    blocks_of(residual)
    y_in(DN, 0)
    down(0, 1, True)

    def f_wait(h):
        with scope("fwait"):
            for q in range(lanes):
                f_copy(q, h).wait_recv()

    f_wait(0)
    ff1(1 - role, 0, fh, 0)

    @pl.when(~edge)
    def _():
        z_in(DN, 1)

    f_wait(1)

    @pl.when(edge)
    def _():
        zsends(DN, mids[1:])
        z_in(DN, 1)

    ff1(1 - role, 0, fh, 1)
    for ev in ((far[0], 0), (0, 0), (0, 1)):
        down(*ev, False)
    pending = [(0, 0), (far[0], 0), (0, 1)]
    done = []
    for k in range(len(far)):
        if k and k + 1 < len(far):
            z_in(DN, far[k + 1])
        y_in(DN, far[k])
        late = [(far[k + 1], 0)] if k + 1 < len(far) else []
        for ev in late + [(far[k], 1)]:
            both(*ev)
            pending.append(ev)
        if late:
            for ev in pending[:2 + k]:
                fold(*ev)
            done += pending[:2 + k]
            pending = pending[2 + k:]
    for ev in pending:
        fold(*ev)
    for ev in done + pending:
        prep(*ev)

    lane = lax.broadcasted_iota(jnp.int32, (rb, 128), 1)

    def gather_up(rs):
        mean = sum(jnp.sum(total[gl, rs, :], axis=1, keepdims=True) for gl in range(per)) / feat
        square = jnp.zeros((rb, 1), f32)
        for gl in range(per):
            v = total[gl, rs, :] - mean
            square = square + jnp.sum(v * v, axis=1, keepdims=True)
        moments[0, rs, :] = jnp.where(lane == 0, mean, jnp.where(lane == 1, square, 0.0))

    with scope("gather_up"):
        blocks_of(gather_up)

    def drain():
        for q in range(lanes):
            for k in range(2):
                x_copy(q, k).wait_send()
                g_copy(q, k).wait_send()
            for h in range(2):
                m_copy(q, h).wait_send()
                f_copy(q, h).wait_send()
        for h in range(2):
            a_copy(h).wait_send()

        def sent(g, carry):
            @pl.when(lax.div(g, per) != t)
            def _():
                r_copy(g, 0).wait_send()
                r_copy(g, 1).wait_send()
            return carry

        lax.fori_loop(0, n, sent, 0)

        def folded(gl, carry):
            p_copy(gl).wait_send()
            return carry

        lax.fori_loop(0, per, folded, 0)
        def gone(sem, w, count):
            if count:
                b = stretch(w, count)
                remote(b, b, sem.at[w], zr_sem.at[w, 0], opp, t).wait_send()

        for w in range(len(streams) if spare else len(streams) - 2):
            if w in extra:
                pl.when(taker)(lambda: gone(zs_sem, w, zn // 2 - 1))
                pl.when(~taker)(lambda: gone(zs_sem, w, zn // 2))
            else:
                gone(zs_sem, w, zn // 2 if w in (WIN, WPO) else zn - 1)

            def rest():
                gone(ys_sem, w, zn)
                gone(ss_sem, w, 2 * zn)
            having(w, taker, rest)
            if w in (WIN, WPO):
                for j in near[1:]:
                    @pl.when(gate(z, across(j)))
                    def _():
                        relay(w, j).wait_send()

    stat[...] = jnp.transpose(moments[0])[0:8, :]
    for q in range(lanes):
        t_copy(q).start()
    drain()
    spread[...] = jnp.zeros_like(spread)
    for q in range(lanes):
        with scope("twait"):
            t_copy(q).wait_recv()
        spread[0:8, :] = srecv[q]
        moments[q + 1] = jnp.transpose(spread[...])

    def last_norm(rs):
        means = [moments[q, rs, 0:1] for q in range(tps)]
        mean = sum(means) / tps
        square = sum(moments[q, rs, 1:2] for q in range(tps))
        for m in means:
            square = square + feat * (m - mean) * (m - mean)
        inv = lax.rsqrt(square / width + norm_eps)
        for gl in range(per):
            cs = slice(gl * rc, (gl + 1) * rc)
            out_ref[rs, cs] = ((total[gl, rs, :] - mean) * inv * gout_ref[0:1, cs]).astype(bf16)

    with scope("norm3"):
        blocks_of(last_norm)

    for q in range(lanes):
        t_copy(q).wait_send()


def local(zn, tps, tokens, gain_mixer, w_in, pool_scale, w_pool_out, gain_mid, w_ff1, w_ff2, gain_out):
    rows, feat = tokens.shape
    own, cin = w_in.shape
    ffw = w_ff1.shape[1]
    fh = (ffw + ffw // 16 // 256 * 256) // 2
    width = feat * tps
    n = zn * 2
    per = n // tps
    rc = own * 2
    vmem, hbm = pl.BlockSpec(memory_space=pltpu.VMEM), pl.BlockSpec(memory_space=pl.ANY)
    dma = pltpu.SemaphoreType.DMA
    lanes = tps - 1
    return pl.pallas_call(
        functools.partial(kernel, zn, tps),
        out_shape=jax.ShapeDtypeStruct((rows, feat), bf16),
        in_specs=[hbm] + [vmem] * 4 + [hbm] * 4,
        out_specs=vmem,
        scratch_shapes=[
            pltpu.VMEM((width, cin), bf16),
            pltpu.VMEM((width, cin), bf16),
            pltpu.VMEM((width, fh), bf16),
            pltpu.VMEM((width, fh), bf16),
            pltpu.VMEM((own, ffw), bf16),
            pltpu.VMEM((own, ffw), bf16),
            pltpu.VMEM((tps, rows, feat), bf16),
            pltpu.VMEM((2, tps, 1, feat), f32),
            pltpu.VMEM((rows, width), bf16),
            pltpu.VMEM((rows, width), bf16),
            pltpu.VMEM((lanes, rows, width), bf16),
            pltpu.VMEM((2, rows, width), bf16),
            pltpu.VMEM((2 * rows, fh), bf16),
            pltpu.VMEM((n, 2 * rows, rc), bf16),
            pltpu.VMEM((lanes, per, 2 * rows, rc), bf16),
            pltpu.VMEM((per, rows, rc), bf16),
            pltpu.VMEM((per, rows, rc), bf16),
            pltpu.VMEM((per, rows, rc), f32),
            pltpu.VMEM((tps, rows, 128), f32),
            pltpu.VMEM((128, rows), f32),
            pltpu.VMEM((8, rows), f32),
            pltpu.VMEM((lanes, 8, rows), f32),
            pltpu.VMEM((rows, cin), f32),
            dma((9,)),
            dma((8,)), dma((2, zn)), dma((8, zn)), dma((8,)), dma((8, zn)), dma((8,)), dma((8,)), dma((zn, 2)),
            dma((lanes, 2)), dma((lanes, 2)), dma((lanes, 2)), dma((lanes, 2)),
            dma((lanes, 2)), dma((lanes, 2)), dma((2,)), dma((2,)), dma((lanes, 2)), dma((lanes, 2)),
            dma((n, 2)), dma((lanes, per, 2)), dma((per,)), dma((per,)), dma((lanes,)), dma((lanes,)),
        ],
        compiler_params=pltpu.CompilerParams(
            collective_id=0, has_side_effects=True, vmem_limit_bytes=67043328
        ),
    )(tokens, gain_mixer[None], gain_mid[None], pool_scale[None], gain_out[None], w_in, w_pool_out, w_ff1, w_ff2)


def solution(mesh):
    zn, tps = mesh.shape["fs"] // 4, mesh.shape["tp"]
    return jax.shard_map(
        functools.partial(local, zn, tps),
        mesh=mesh,
        in_specs=(
            P("fs", "tp"),
            P("tp"),
            P("fs", "tp"),
            P("tp"),
            P("fs", "tp"),
            P("tp"),
            P("fs", "tp"),
            P("fs", "tp"),
            P("tp"),
        ),
        out_specs=P("fs", "tp"),
        check_vma=False,
    )
```
